32 devices in a mesh: ep: 8 (over z, x), tp: 4 (over y, core).
Axes of the slice: x: 2, y: 2, z: 4, core: 2. Of those that a mesh axis runs over, the one named last changes fastest.
Arguments:
- hidden_in: bfloat16 [128, 1024], P('ep'), may hold values from -6 to 6
- attn_gain: float32 [1024], replicated, may hold values from 0.1 to 1.9
- w_qdown: bfloat16 [1024, 256], replicated, may hold values from -0.1875 to 0.1875
- q_gain: float32 [256], replicated, may hold values from 0.1 to 1.9
- w_qnope: bfloat16 [256, 512], replicated, may hold values from -0.375 to 0.375
- w_qrope: bfloat16 [256, 256], replicated, may hold values from -0.375 to 0.375
- w_kvdown: bfloat16 [1024, 128], replicated, may hold values from -0.1875 to 0.1875
- kv_gain: float32 [128], replicated, may hold values from 0.1 to 1.9
- w_krope: bfloat16 [1024, 32], replicated, may hold values from -0.1875 to 0.1875
- w_ukey: bfloat16 [128, 512], replicated, may hold values from -0.75 to 0.75
- w_uvalue: bfloat16 [128, 512], replicated, may hold values from -0.5 to 0.5
- w_out: bfloat16 [512, 1024], P('tp'), may hold values from -0.25 to 0.25
- cache_latent: bfloat16 [128, 1024, 128], P(('ep', 'tp')), may hold values from -6 to 6
- cache_rope: bfloat16 [128, 32, 1024], P(('ep', 'tp')), may hold values from -900 to 900
- lengths: int32 [128], P(('ep', 'tp')), may hold values from 1 to 1024, as said below
- ffn_gain: float32 [1024], replicated, may hold values from 0.1 to 1.9
- routes: int32 [128, 2], P('ep'), may hold values from 0 to 3, all different within a row; in each aligned block of 16 rows (0 to 15, 16 to 31, ...) at most 16 rows name the same one
- route_weights: float32 [128, 2], P('ep'), may hold values from 0.25 to 1
- w_gate: bfloat16 [8, 1024, 1792], P('ep', None, 'tp'), may hold values from -0.1875 to 0.1875
- w_up: bfloat16 [8, 1024, 1792], P('ep', None, 'tp'), may hold values from -0.1875 to 0.1875
- w_down: bfloat16 [8, 1792, 1024], P('ep', 'tp'), may hold values from -0.09375 to 0.09375
Outputs:
- next_hidden: bfloat16 [128, 1024], P('ep', 'tp')
The draws below stay inside these ranges and needn't reach their ends.
Inputs may be any that keep to these rules, and one draw needn't show every extreme that they name: `lengths`: each sequence has 1 to 1024 valid cached positions; in every aligned block of 16 sequences one has all 1024. `routes`: each row names two different experts. In the aligned blocks of 16 rows no expert is named by more than 16 rows, and in some block one expert is named by exactly 16.
All inputs are finite; a program needn't handle non-finite values.
Results may differ from the reference program's by a relative error of at most 0.014.
The reference program's roundings to bfloat16 on the way count: a program that leaves them out, or rounds other values in their place, can miss the bound.
Values may be sent and summed in bfloat16 or wider, within the bound.
A program may use at most 64 MiB of HBM per device.

```python
import math
import jax
import jax.numpy as jnp
import numpy as np
from jax import lax

D = 1024
HEADS = 8
NOPE = 64
ROPE = 32
VDIM = 64
QLORA = 256
KVLORA = 128
EXPERT_FF = 3584
CACHE = 1024
FF_HALF = 1792
SEQ_GRP = 16
TOKENS = 128
EXPERTS = 4
UNITS = 8
CAP = 16
N_EP = 8
N_TP = 4


def draw_lengths(key, part):
    key_set = jax.random.split(key, 4)
    longer = jax.random.randint(key_set[0], (TOKENS,), 1, CACHE + 1)
    shorter = jax.random.randint(key_set[1], (TOKENS,), 1, 9)
    chosen_short = jax.random.randint(key_set[2], (TOKENS,), 0, 2) == 0
    merged = jnp.where(chosen_short, shorter, longer).reshape(TOKENS // SEQ_GRP, SEQ_GRP)
    full_slot = jax.random.randint(key_set[3], (TOKENS // SEQ_GRP, 1), 0, SEQ_GRP)
    marked = jnp.arange(SEQ_GRP)[None, :] == full_slot
    return jnp.where(marked, CACHE, merged).reshape(TOKENS).astype(jnp.int32)


def draw_cache_rope(key, part):
    key_pair = jax.random.split(key, 1)
    values = jnp.clip(jax.random.normal(key_pair[0], (TOKENS, ROPE, CACHE), jnp.float32), -6.0, 6.0)
    return values.astype(jnp.bfloat16)


def steps_of(rng, dims, shards, least, largest):
    factor_of = 1.0
    for position, blocks in shards:
        heights = jax.random.uniform(jax.random.fold_in(jax.random.fold_in(rng, 6), position), (blocks,), jnp.float32, least / len(shards), largest / len(shards))
        factor_of = factor_of * jnp.repeat(jnp.exp(heights), dims[position] // blocks).reshape((-1,) + (1,) * (len(dims) - 1 - position))
    return factor_of


def assign_block(key, own, number, rows, amount, top, most, skew):
    sequence = jax.random.permutation(key, amount)
    packed, common = load_shares(amount, rows * top, most, skew, True), load_shares(amount, rows * top, most, skew, False)
    places = jnp.arange(amount)

    def named(sizes, rotation):
        used = int((sizes > 0).sum())
        fixed = max(1, used // 4)
        moved = fixed + (places - fixed + rotation * (used - fixed)) % max(1, amount - fixed)
        return jnp.zeros((amount,), jnp.int32).at[sequence[jnp.where(places < fixed, places, moved)]].set(jnp.asarray(sizes, jnp.int32))

    sizes = jnp.where(number % 4 == 0, named(packed, number // 4), named(common, number - number // 4 - 1))
    mixed = jax.random.permutation(jax.random.fold_in(own, 3), amount)
    giver, taker = mixed[0:amount // 2 * 2:2], mixed[1:amount // 2 * 2:2]
    slack = jnp.minimum(sizes[giver] - 1, most - sizes[taker]) // 2
    slack = jnp.where((giver == sequence[0]) | (taker == sequence[0]) | (sizes[taker] == 0), 0, jnp.maximum(slack, 0))
    moved = jax.random.randint(jax.random.fold_in(own, 4), (amount // 2,), 0, 1 << 20) % (slack + 1)
    sizes = sizes.at[giver].add(-moved).at[taker].add(moved)
    members = jnp.searchsorted(jnp.cumsum(sizes), jnp.arange(rows * top), side="right").astype(jnp.int32)
    grid = members.reshape(top, rows).T
    grid = grid[jax.random.permutation(jax.random.fold_in(own, 1), rows)]
    rotation = jax.random.randint(jax.random.fold_in(own, 2), (rows, 1), 0, top)
    return jnp.take_along_axis(grid, (jnp.arange(top)[None, :] + rotation) % top, axis=1)


def load_shares(count, total, limit, slope, full):
    weights = [(1 << 20) // math.isqrt(grade ** slope) + 1 for grade in range(1, count + 1)]
    largest = limit if full else min(limit, max(-(-total // count), total * weights[0] // sum(weights)))
    least = 1 if total - largest >= count - 1 else 0
    counts, rest = [largest] + [least] * (count - 1), total - largest - least * (count - 1)
    while rest > 0:
        movable = [i for i in range(1, count) if counts[i] < largest] or [i for i in range(1, count) if counts[i] < limit]
        mass, left = sum([weights[i] for i in movable]), rest
        for i in movable:
            addition = min(limit - counts[i], max(1, left * weights[i] // mass), rest)
            counts[i] = counts[i] + addition
            rest = rest - addition
    return np.array(counts)


def gaussian(own_key, extent, deviation, reach, shards=(), kind=jnp.bfloat16):
    level = steps_of(own_key, extent, shards, -0.22, 0.18) if shards else 1.0
    array = jax.random.normal(own_key, extent, jnp.float32) * deviation * level
    return jnp.minimum(jnp.maximum(array, -reach), reach).astype(kind)


def setup_inputs(seed: int = 0) -> dict:
    key_list = jax.random.split(jax.random.key(seed), 22)
    hidden_in = gaussian(key_list[0], (TOKENS, D), 1.0, 6.0, ((0, 8),))
    attn_gain = jnp.clip(1.0 + 0.18 * jax.random.normal(key_list[1], (D,), jnp.float32), 0.1, 1.9)
    w_qdown = gaussian(key_list[2], (D, QLORA), D ** -0.5, 0.1875)
    q_gain = jnp.clip(1.0 + 0.18 * jax.random.normal(key_list[3], (QLORA,), jnp.float32), 0.1, 1.9)
    w_qnope = gaussian(key_list[4], (QLORA, HEADS * NOPE), QLORA ** -0.5, 0.375)
    w_qrope = gaussian(key_list[5], (QLORA, HEADS * ROPE), QLORA ** -0.5, 0.375)
    w_kvdown = gaussian(key_list[6], (D, KVLORA), D ** -0.5, 0.1875)
    kv_gain = jnp.clip(1.0 + 0.18 * jax.random.normal(key_list[7], (KVLORA,), jnp.float32), 0.1, 1.9)
    w_krope = gaussian(key_list[8], (D, ROPE), D ** -0.5, 0.1875)
    w_ukey = gaussian(key_list[9], (KVLORA, HEADS * NOPE), NOPE ** -0.5, 0.75)
    w_uvalue = gaussian(key_list[10], (KVLORA, HEADS * VDIM), KVLORA ** -0.5, 0.5)
    w_out = gaussian(key_list[11], (HEADS * VDIM, D), (HEADS * VDIM) ** -0.5, 0.25, ((0, 4),))
    cache_latent = gaussian(key_list[12], (TOKENS, CACHE, KVLORA), 1.0, 6.0, ((0, 32),))
    cache_rope = draw_cache_rope(jax.random.fold_in(key_list[21], 71), 0)
    lengths = draw_lengths(jax.random.fold_in(key_list[21], 71), 0)
    ffn_gain = jnp.clip(1.0 + 0.18 * jax.random.normal(key_list[15], (D,), jnp.float32), 0.1, 1.9)
    routes_keys = jax.random.split(jax.random.fold_in(key_list[16], 1), TOKENS // SEQ_GRP)
    routes_turns = jax.random.permutation(jax.random.fold_in(key_list[16], 3), TOKENS // SEQ_GRP)
    routes = jax.vmap(lambda own, number: assign_block(jax.random.fold_in(key_list[16], 2), own, number, SEQ_GRP, EXPERTS, 2, CAP, 2))(routes_keys, routes_turns).reshape((TOKENS, 2))
    route_weights = jnp.clip(0.25 + 0.75 * jax.random.uniform(key_list[17], (TOKENS, 2), jnp.float32) ** steps_of(key_list[17], (TOKENS, 2), ((0, 8),), -0.2, 0.2), 0.25, 1.0)
    w_gate = gaussian(key_list[18], (UNITS, D, FF_HALF), D ** -0.5, 0.1875, ((0, 8), (2, 4)))
    w_up = gaussian(key_list[19], (UNITS, D, FF_HALF), D ** -0.5, 0.1875, ((0, 8), (2, 4)))
    w_down = gaussian(key_list[20], (UNITS, FF_HALF, D), EXPERT_FF ** -0.5, 0.09375, ((0, 8), (1, 4)))
    return dict(hidden_in=hidden_in, attn_gain=attn_gain, w_qdown=w_qdown, q_gain=q_gain, w_qnope=w_qnope, w_qrope=w_qrope, w_kvdown=w_kvdown, kv_gain=kv_gain, w_krope=w_krope, w_ukey=w_ukey, w_uvalue=w_uvalue, w_out=w_out, cache_latent=cache_latent, cache_rope=cache_rope, lengths=lengths, ffn_gain=ffn_gain, routes=routes, route_weights=route_weights, w_gate=w_gate, w_up=w_up, w_down=w_down)


eps = 1e-06
rope_base = 10000.0

def rms_scale(values, gain):
    return values * lax.rsqrt(lax.optimization_barrier(jnp.mean(values * values, axis=-1, keepdims=True)) + eps) * gain

def rotate(values, positions):
    width = values.shape[-1]
    middle = width // 2
    inverse = jnp.power(rope_base, -jnp.arange(0, width, 2).astype(jnp.float32) / width)
    angles = positions.astype(jnp.float32)[:, None] * inverse[None, :]
    angles = jnp.concatenate([angles, angles], axis=-1)
    target = (angles.shape[0],) + (1,) * (values.ndim - 2) + (width,)
    cosine = jnp.cos(angles).reshape(target)
    sine = jnp.sin(angles).reshape(target)
    turned = jnp.concatenate([-values[..., middle:], values[..., :middle]], axis=-1)
    return values * cosine + turned * sine

def route_slots(route_table, expert_count):
    flat_ids = route_table.reshape(-1)
    onehot = (flat_ids[:, None] == jnp.arange(expert_count, dtype=jnp.int32)[None, :]).astype(jnp.int32)
    before = jnp.cumsum(onehot, axis=0) - onehot
    return lax.optimization_barrier(jnp.sum(before * onehot, axis=1)).reshape(route_table.shape).astype(jnp.int32)

def reference(hidden_in, attn_gain, w_qdown, q_gain, w_qnope, w_qrope, w_kvdown, kv_gain, w_krope, w_ukey, w_uvalue, w_out, cache_latent, cache_rope, lengths, ffn_gain, routes, route_weights, w_gate, w_up, w_down):
    score_scale = (NOPE + ROPE) ** (-0.5)
    head_block = HEADS * VDIM // N_TP
    key_table = w_ukey.reshape(KVLORA, HEADS, NOPE).astype(jnp.float32)
    value_table = w_uvalue.reshape(KVLORA, HEADS, VDIM).astype(jnp.float32)

    def attend(group_block):
        group_rows, latents, rotated, valid_len = group_block
        normed = rms_scale(group_rows.astype(jnp.float32), attn_gain).astype(jnp.bfloat16)
        q_small = rms_scale(jnp.dot(normed, w_qdown, preferred_element_type=jnp.float32), q_gain).astype(jnp.bfloat16)
        q_plain = jnp.dot(q_small, w_qnope, preferred_element_type=jnp.float32).astype(jnp.bfloat16).reshape(-1, HEADS, NOPE)
        q_turned = rotate(jnp.dot(q_small, w_qrope, preferred_element_type=jnp.float32).reshape(-1, HEADS, ROPE), valid_len).astype(jnp.bfloat16)
        q_latent = jnp.einsum('shn,chn->shc', q_plain.astype(jnp.float32), key_table).astype(jnp.bfloat16)
        new_latent = rms_scale(jnp.dot(normed, w_kvdown, preferred_element_type=jnp.float32), kv_gain).astype(jnp.bfloat16)
        new_rope = rotate(jnp.dot(normed, w_krope, preferred_element_type=jnp.float32), valid_len).astype(jnp.bfloat16)
        past_scores = (jnp.einsum('shc,spc->shp', q_latent.astype(jnp.float32), latents.astype(jnp.float32)) + jnp.einsum('shr,srp->shp', q_turned.astype(jnp.float32), rotated.astype(jnp.float32))) * score_scale
        in_range = jnp.arange(CACHE)[None, None, :] < valid_len[:, None, None]
        past_scores = jnp.where(in_range, past_scores, -1e+30)
        fresh_score = (lax.optimization_barrier(jnp.sum(q_latent.astype(jnp.float32) * new_latent.astype(jnp.float32)[:, None, :], axis=-1)) + lax.optimization_barrier(jnp.sum(q_turned.astype(jnp.float32) * new_rope.astype(jnp.float32)[:, None, :], axis=-1))) * score_scale
        highest = jnp.maximum(lax.optimization_barrier(jnp.max(past_scores, axis=-1)), fresh_score)
        past_exp = jnp.exp(past_scores - highest[..., None])
        fresh_exp = jnp.exp(fresh_score - highest)
        divisor = lax.optimization_barrier(jnp.sum(past_exp, axis=-1)) + fresh_exp
        past_prob = (past_exp / divisor[..., None]).astype(jnp.bfloat16)
        fresh_prob = (fresh_exp / divisor).astype(jnp.bfloat16)
        latent_mix = (jnp.einsum('shp,spc->shc', past_prob.astype(jnp.float32), latents.astype(jnp.float32)) + fresh_prob.astype(jnp.float32)[..., None] * new_latent.astype(jnp.float32)[:, None, :]).astype(jnp.bfloat16)
        head_values = jnp.einsum('shc,chv->shv', latent_mix.astype(jnp.float32), value_table).astype(jnp.bfloat16).reshape(-1, HEADS * VDIM)
        attended = jnp.zeros((head_values.shape[0], D), jnp.float32)
        for device in range(N_TP):
            block_term = jnp.dot(head_values[:, device * head_block:(device + 1) * head_block], w_out[device * head_block:(device + 1) * head_block], preferred_element_type=jnp.float32)
            attended = attended + lax.optimization_barrier(block_term.astype(jnp.bfloat16)).astype(jnp.float32)
        return attended
    attended = lax.map(attend, (hidden_in.reshape(N_EP, SEQ_GRP, D), cache_latent.reshape(N_EP, SEQ_GRP, CACHE, KVLORA), cache_rope.reshape(N_EP, SEQ_GRP, ROPE, CACHE), lengths.reshape(N_EP, SEQ_GRP))).reshape(TOKENS, D)
    residual = hidden_in.astype(jnp.float32) + attended
    normed_two = rms_scale(residual, ffn_gain).astype(jnp.bfloat16)
    group_input = normed_two.reshape(N_EP, SEQ_GRP, D)
    group_routes = routes.reshape(N_EP, SEQ_GRP, 2)
    group_slots = jax.vmap(lambda table: route_slots(table, EXPERTS))(group_routes)
    quarter_ff = FF_HALF // N_TP
    slot_range = jnp.arange(CAP, dtype=jnp.int32)

    def serve_unit(unit):
        expert = unit // 2
        chosen = (group_routes == expert)[:, None, :, :] & (group_slots[:, None, :, :] == slot_range[None, :, None, None])
        chooser = lax.optimization_barrier(jnp.sum(chosen.astype(jnp.float32), axis=-1))
        arrived = jnp.einsum('gcr,grd->gcd', chooser, group_input.astype(jnp.float32)).astype(jnp.bfloat16).reshape(N_EP * CAP, D)
        gate_part = jnp.dot(arrived, w_gate[unit], preferred_element_type=jnp.float32)
        up_part = jnp.dot(arrived, w_up[unit], preferred_element_type=jnp.float32)
        inner = (jax.nn.silu(gate_part) * up_part).astype(jnp.bfloat16)
        down_table = w_down[unit]
        summed = jnp.zeros((N_EP * CAP, D), jnp.float32)
        for device in range(N_TP):
            block_term = jnp.dot(inner[:, device * quarter_ff:(device + 1) * quarter_ff], down_table[device * quarter_ff:(device + 1) * quarter_ff], preferred_element_type=jnp.float32)
            summed = summed + lax.optimization_barrier(block_term.astype(jnp.bfloat16)).astype(jnp.float32)
        return summed.astype(jnp.bfloat16).reshape(N_EP, CAP, D)
    unit_out = lax.map(serve_unit, jnp.arange(UNITS, dtype=jnp.int32))
    group_index = jnp.arange(N_EP, dtype=jnp.int32)[:, None, None]
    first_half = unit_out[2 * group_routes, group_index, group_slots].astype(jnp.float32)
    second_half = unit_out[2 * group_routes + 1, group_index, group_slots].astype(jnp.float32)
    blended = lax.optimization_barrier(jnp.sum(route_weights.reshape(N_EP, SEQ_GRP, 2)[..., None] * (first_half + second_half), axis=2))
    return (residual + blended.reshape(TOKENS, D)).astype(jnp.bfloat16)
```

```python
import functools

import jax
import jax.numpy as jnp
import numpy as np
from jax import lax
from jax.experimental import pallas as pl
from jax.experimental.pallas import tpu as pltpu
from jax.sharding import PartitionSpec as P

HEADS = 8
NOPE = 64
ROPE = 32
VDIM = 64
KVLORA = 128


eps = 1e-06
rope_base = 10000.0


def rms_scale(values, gain):
    return values * lax.rsqrt(jnp.mean(values * values, axis=-1, keepdims=True) + eps) * gain


def rotate(values, positions):
    width = values.shape[-1]
    middle = width // 2
    inverse = jnp.power(rope_base, -jnp.arange(0, width, 2).astype(jnp.float32) / width)
    angles = positions.astype(jnp.float32)[:, None] * inverse[None, :]
    angles = jnp.concatenate([angles, angles], axis=-1)
    target = (angles.shape[0],) + (1,) * (values.ndim - 2) + (width,)
    cosine = jnp.cos(angles).reshape(target)
    sine = jnp.sin(angles).reshape(target)
    turned = jnp.concatenate([-values[..., middle:], values[..., :middle]], axis=-1)
    return values * cosine + turned * sine


def route_slots(route_table, expert_count):
    flat_ids = route_table.reshape(-1)
    onehot = (flat_ids[:, None] == jnp.arange(expert_count, dtype=jnp.int32)[None, :]).astype(
        jnp.int32
    )
    before = jnp.cumsum(onehot, axis=0) - onehot
    return jnp.sum(before * onehot, axis=1).reshape(route_table.shape)


def unit_block(arrived, w_gate, w_up, w_down):
    gate_part = jnp.einsum("scd,df->scf", arrived, w_gate[0], preferred_element_type=jnp.float32)
    up_part = jnp.einsum("scd,df->scf", arrived, w_up[0], preferred_element_type=jnp.float32)
    inner = (jax.nn.silu(gate_part) * up_part).astype(jnp.bfloat16)
    block_term = jnp.einsum("scf,fd->scd", inner, w_down[0], preferred_element_type=jnp.float32)
    summed = lax.psum_scatter(
        block_term.astype(jnp.bfloat16), "tp", scatter_dimension=2, tiled=True
    )
    return lax.all_to_all(summed, "ep", split_axis=0, concat_axis=0, tiled=True)


def per_device(
    hidden_in,
    attn_gain,
    w_qdown,
    q_gain,
    w_qnope,
    w_qrope,
    w_kvdown,
    kv_gain,
    w_krope,
    w_ukey,
    w_uvalue,
    w_out,
    cache_latent,
    cache_rope,
    lengths,
    ffn_gain,
    routes,
    route_weights,
    w_gate,
    w_up,
    w_down,
):
    group_rows, width = hidden_in.shape
    own_count = lengths.shape[0]
    tp_rank = lax.axis_index("tp")
    score_scale = (NOPE + ROPE) ** (-0.5)
    own_rows = lax.dynamic_slice_in_dim(hidden_in, tp_rank * own_count, own_count, 0).astype(
        jnp.float32
    )
    normed = rms_scale(own_rows, attn_gain).astype(jnp.bfloat16)
    q_small = rms_scale(
        jnp.dot(normed, w_qdown, preferred_element_type=jnp.float32), q_gain
    ).astype(jnp.bfloat16)
    q_plain = (
        jnp.dot(q_small, w_qnope, preferred_element_type=jnp.float32)
        .astype(jnp.bfloat16)
        .reshape(own_count, HEADS, NOPE)
    )
    q_turned = rotate(
        jnp.dot(q_small, w_qrope, preferred_element_type=jnp.float32).reshape(
            own_count, HEADS, ROPE
        ),
        lengths,
    ).astype(jnp.bfloat16)
    q_latent = jnp.einsum(
        "shn,chn->shc",
        q_plain,
        w_ukey.reshape(KVLORA, HEADS, NOPE),
        preferred_element_type=jnp.float32,
    ).astype(jnp.bfloat16)
    new_latent = rms_scale(
        jnp.dot(normed, w_kvdown, preferred_element_type=jnp.float32), kv_gain
    ).astype(jnp.bfloat16)
    new_rope = rotate(jnp.dot(normed, w_krope, preferred_element_type=jnp.float32), lengths).astype(
        jnp.bfloat16
    )
    past_scores = (
        jnp.einsum("shc,spc->shp", q_latent, cache_latent, preferred_element_type=jnp.float32)
        + jnp.einsum("shr,srp->shp", q_turned, cache_rope, preferred_element_type=jnp.float32)
    ) * score_scale
    in_range = jnp.arange(cache_latent.shape[1])[None, None, :] < lengths[:, None, None]
    past_scores = jnp.where(in_range, past_scores, -1e30)
    fresh_score = (
        jnp.einsum("shc,sc->sh", q_latent, new_latent, preferred_element_type=jnp.float32)
        + jnp.einsum("shr,sr->sh", q_turned, new_rope, preferred_element_type=jnp.float32)
    ) * score_scale
    highest = jnp.maximum(jnp.max(past_scores, axis=-1), fresh_score)
    past_exp = jnp.exp(past_scores - highest[..., None])
    fresh_exp = jnp.exp(fresh_score - highest)
    divisor = jnp.sum(past_exp, axis=-1) + fresh_exp
    past_prob = (past_exp / divisor[..., None]).astype(jnp.bfloat16)
    fresh_prob = (fresh_exp / divisor).astype(jnp.bfloat16)
    latent_mix = (
        jnp.einsum("shp,spc->shc", past_prob, cache_latent, preferred_element_type=jnp.float32)
        + fresh_prob.astype(jnp.float32)[..., None] * new_latent.astype(jnp.float32)[:, None, :]
    ).astype(jnp.bfloat16)
    head_values = (
        jnp.einsum(
            "shc,chv->shv",
            latent_mix,
            w_uvalue.reshape(KVLORA, HEADS, VDIM),
            preferred_element_type=jnp.float32,
        )
        .astype(jnp.bfloat16)
        .reshape(own_count, HEADS * VDIM)
    )
    by_heads = lax.all_to_all(head_values, "tp", split_axis=1, concat_axis=0, tiled=True)
    attended = lax.psum(
        jnp.dot(by_heads, w_out, preferred_element_type=jnp.float32).astype(jnp.bfloat16), "tp"
    ).astype(jnp.float32)
    residual = hidden_in.astype(jnp.float32) + attended
    normed_two = rms_scale(residual, ffn_gain).astype(jnp.bfloat16)
    unit_count = lax.axis_size("ep")
    expert_count = unit_count // 2
    capacity = max(2, 4 * group_rows // expert_count)
    quarter = width // lax.axis_size("tp")
    slots = route_slots(routes, expert_count)
    expert_of_unit = jnp.arange(unit_count, dtype=jnp.int32) // 2
    slot_range = jnp.arange(capacity, dtype=jnp.int32)
    chosen = (routes[None, None, :, :] == expert_of_unit[:, None, None, None]) & (
        slots[None, None, :, :] == slot_range[None, :, None, None]
    )
    chooser = jnp.sum(chosen.astype(jnp.int32), axis=-1).astype(jnp.bfloat16)
    outgoing = jnp.einsum(
        "ucr,rd->ucd", chooser, normed_two, preferred_element_type=jnp.float32
    ).astype(jnp.bfloat16)
    returned = unit_block(
        lax.all_to_all(outgoing, "ep", split_axis=0, concat_axis=0, tiled=True),
        w_gate,
        w_up,
        w_down,
    )
    stacked = returned.reshape(unit_count * capacity, quarter)
    first_row = routes * (2 * capacity) + slots
    first_half = stacked[first_row].astype(jnp.float32)
    second_half = stacked[first_row + capacity].astype(jnp.float32)
    blended = jnp.sum(route_weights[..., None] * (first_half + second_half), axis=1)
    own_columns = lax.dynamic_slice_in_dim(residual, tp_rank * quarter, quarter, 1)
    return (own_columns + blended).astype(jnp.bfloat16)


LINK = pl.DeviceIdType.MESH
F32 = jnp.float32
BF16 = jnp.bfloat16


def mm(a, b):
    return jnp.dot(a, b, preferred_element_type=F32)


def mm_nt(a, b):
    return lax.dot_general(a, b, (((1,), (1,)), ((), ())), preferred_element_type=F32)


def iota(shape, dim):
    return lax.broadcasted_iota(jnp.int32, shape, dim)


def layer_kernel(groups, lanes_tp, *refs):
    names = 22
    hbm, out_ref = refs[:names], refs[names]
    local = refs[names + 1 : 2 * names + 1]
    (
        load_sem, hv_send, hv_recv, rows_buf, part, res_buf, x_buf, y_send, y_recv,
        hv_ss, hv_rs, part_ss, part_rs, x_ss, x_rs, y_ss, y_rs,
    ) = refs[2 * names + 1 :]
    (
        hidden, attn_gain, w_qdown, q_gain, w_qnope, w_qrope, w_kvdown, kv_gain, w_krope,
        w_ukey, w_uvalue, w_out, cache_latent, cache_rope, lengths, ffn_gain, routes,
        route_weights, w_gate, w_up, w_down, inverse,
    ) = local
    g, t = lax.axis_index("ep"), lax.axis_index("tp")
    devices = groups * lanes_tp
    me = g * lanes_tp + t

    barrier = pltpu.get_barrier_semaphore()

    def greet(step, carry):
        peer = lax.rem(me + step, devices)
        pl.semaphore_signal(
            barrier, inc=1, device_id=(peer // lanes_tp, lax.rem(peer, lanes_tp)),
            device_id_type=LINK,
        )
        return carry

    lax.fori_loop(1, devices, greet, 0)

    loads = [
        pltpu.make_async_copy(hbm[i], local[i], load_sem.at[i]) for i in range(names)
    ]
    order = [0, 1, 2, 3, 14, 21, 6, 8, 7, 4, 5, 9, 12, 13, 10, 11, 15, 16, 17, 18, 19, 20]
    for i in order:
        loads[i].start()

    own = lengths.shape[0]
    rows, width = hidden.shape
    quarter = width // lanes_tp
    pad = 8

    for i in (0, 1, 2, 3):
        loads[i].wait()
    pick = (iota((pad, rows), 1) == iota((pad, rows), 0) + t * own) & (
        iota((pad, rows), 0) < own
    )
    mine = mm(jnp.where(pick, 1.0, 0.0).astype(BF16), hidden[...])
    normed = rms_scale(mine, attn_gain[...]).astype(BF16)
    q_small = rms_scale(mm(normed, w_qdown[...]), q_gain[...]).astype(BF16)
    for i in (14, 21, 6, 8, 7, 4, 5):
        loads[i].wait()
    position = jnp.zeros((pad, 1), jnp.int32)
    for s in range(own):
        position = jnp.where(iota((pad, 1), 0) == s, lengths[s], position)
    angles = position.astype(F32) * inverse[...]
    cosine, sine = jnp.cos(angles), jnp.sin(angles)
    new_latent = rms_scale(mm(normed, w_kvdown[...]), kv_gain[...]).astype(BF16).astype(F32)
    rope_key = mm(normed, w_krope[...])
    turned_key = jnp.concatenate([-rope_key[:, ROPE // 2 :], rope_key[:, : ROPE // 2]], axis=1)
    new_rope = rope_key * cosine[:, :ROPE] + turned_key * sine[:, :ROPE]
    new_rope = new_rope.astype(BF16).astype(F32)
    q_plain = mm(q_small, w_qnope[...]).astype(BF16).astype(F32)
    q_rope = mm(q_small, w_qrope[...])
    span = HEADS * ROPE
    first = (iota((pad, span), 1) & (ROPE - 1)) < ROPE // 2
    turned = jnp.where(
        first, -pltpu.roll(q_rope, span - ROPE // 2, 1), pltpu.roll(q_rope, ROPE // 2, 1)
    )
    q_turned = (q_rope * cosine + turned * sine).astype(BF16).astype(F32)
    plain_mask = iota((HEADS, HEADS * NOPE), 1) // NOPE == iota((HEADS, HEADS * NOPE), 0)
    rope_mask = iota((HEADS, span), 1) // ROPE == iota((HEADS, span), 0)
    plain_rows = jnp.concatenate(
        [jnp.where(plain_mask, q_plain[s : s + 1, :], 0.0) for s in range(own)], axis=0
    ).astype(BF16)
    rope_rows = jnp.concatenate(
        [jnp.where(rope_mask, q_turned[s : s + 1, :], 0.0) for s in range(own)], axis=0
    ).astype(BF16)
    fold = ((iota((span, ROPE), 0) & (ROPE - 1)) == iota((span, ROPE), 1)).astype(F32)
    q_heads = mm(rope_rows, fold.astype(BF16))
    loads[9].wait()
    q_latent = mm_nt(plain_rows, w_ukey[...]).astype(BF16)
    loads[12].wait()
    loads[13].wait()
    scale = (NOPE + ROPE) ** (-0.5)
    cache = cache_latent.shape[1]
    mixes = []
    for s in range(own):
        heads = slice(s * HEADS, (s + 1) * HEADS)
        ql, qr = q_latent[heads], q_heads[heads]
        scores = (mm_nt(ql, cache_latent[s]) + mm(qr.astype(BF16), cache_rope[s])) * scale
        scores = jnp.where(iota((HEADS, cache), 1) < lengths[s], scores, -1e30)
        fresh = (
            jnp.sum(ql.astype(F32) * new_latent[s : s + 1, :], axis=1, keepdims=True)
            + jnp.sum(qr * new_rope[s : s + 1, :], axis=1, keepdims=True)
        ) * scale
        highest = jnp.maximum(jnp.max(scores, axis=1, keepdims=True), fresh)
        past_exp = jnp.exp(scores - highest)
        fresh_exp = jnp.exp(fresh - highest)
        divisor = jnp.sum(past_exp, axis=1, keepdims=True) + fresh_exp
        past_prob = (past_exp / divisor).astype(BF16)
        fresh_prob = (fresh_exp / divisor).astype(BF16).astype(F32)
        mixes.append(mm(past_prob, cache_latent[s]) + fresh_prob * new_latent[s : s + 1, :])
    loads[10].wait()
    mix = jnp.concatenate(mixes, axis=0).astype(BF16)
    values = mm(mix, w_uvalue[...])
    value_mask = iota((HEADS, HEADS * VDIM), 1) // VDIM == iota((HEADS, HEADS * VDIM), 0)
    block = HEADS * VDIM // lanes_tp
    for s in range(own):
        row = jnp.sum(
            jnp.where(value_mask, values[s * HEADS : (s + 1) * HEADS], 0.0), axis=0, keepdims=True
        )
        row = row.astype(BF16).astype(F32)
        for i in range(lanes_tp):
            hv_send[i, s : s + 1, :] = row[:, i * block : (i + 1) * block]

    pl.semaphore_wait(barrier, devices - 1)

    def hv_copy(peer, slot):
        return pltpu.make_async_remote_copy(
            hv_send.at[peer], hv_recv.at[slot], hv_ss.at[peer], hv_rs.at[slot],
            device_id=(g, peer), device_id_type=LINK,
        )

    peers = [lax.rem(t + i, lanes_tp) for i in range(1, lanes_tp)]
    for peer in peers:
        hv_copy(peer, t).start()
    hv_recv[t] = hv_send[t]
    loads[11].wait()
    loads[15].wait()
    for peer in peers:
        hv_copy(peer, peer).wait_recv()
    for i in range(lanes_tp):
        rows_buf[i * own : (i + 1) * own, :] = hv_recv[i, :own, :]
    part[t] = mm(rows_buf[...].astype(BF16), w_out[...]).astype(BF16)

    def part_copy(peer, slot):
        return pltpu.make_async_remote_copy(
            part.at[slot], part.at[slot], part_ss.at[peer], part_rs.at[slot],
            device_id=(g, peer), device_id_type=LINK,
        )

    for peer in peers:
        part_copy(peer, t).start()
    for peer in peers:
        part_copy(peer, peer).wait_recv()
    attended = part[0].astype(F32)
    for i in range(1, lanes_tp):
        attended = attended + part[i].astype(F32)
    residual = hidden[...].astype(F32) + attended
    normed_two = rms_scale(residual, ffn_gain[...]).astype(BF16)
    for i in range(lanes_tp):
        x_buf[g, i] = normed_two[:, i * quarter : (i + 1) * quarter]
        res_buf[i] = residual[:, i * quarter : (i + 1) * quarter]

    def x_copy(other_g, other_t, slot_g, slot_t):
        return pltpu.make_async_remote_copy(
            x_buf.at[slot_g, slot_t], x_buf.at[slot_g, slot_t],
            x_ss.at[other_g, other_t], x_rs.at[slot_g, slot_t],
            device_id=(other_g, other_t), device_id_type=LINK,
        )

    def others(step):
        return lax.rem(g + 1 + step // lanes_tp, groups), lax.rem(t + step, lanes_tp)

    far = (groups - 1) * lanes_tp

    def x_start(step, carry):
        a, b = others(step)
        x_copy(a, b, g, t).start()
        return carry

    lax.fori_loop(0, far, x_start, 0)
    for i in (16, 17, 18, 19, 20):
        loads[i].wait()

    def x_wait(step, carry):
        a, b = others(step)
        x_copy(a, b, a, b).wait_recv()
        return carry

    lax.fori_loop(0, far, x_wait, 0)

    tokens = groups * rows
    gate = jnp.zeros((tokens, w_gate.shape[2]), F32)
    up = jnp.zeros((tokens, w_gate.shape[2]), F32)
    for i in range(lanes_tp):
        piece = x_buf[:, i].reshape(tokens, quarter)
        depth = slice(i * quarter, (i + 1) * quarter)
        gate = gate + mm(piece, w_gate[0, depth, :])
        up = up + mm(piece, w_up[0, depth, :])
    inner = (gate / (1.0 + jnp.exp(-gate)) * up).astype(BF16)
    for i in range(lanes_tp):
        term = mm(inner, w_down[0, :, i * quarter : (i + 1) * quarter]).astype(BF16)
        y_send[:, i] = term.reshape(groups, rows, quarter)

    def y_copy(other_g, other_t, slot_g, slot_t):
        return pltpu.make_async_remote_copy(
            y_send.at[other_g, other_t], y_recv.at[slot_g, slot_t],
            y_ss.at[other_g, other_t], y_rs.at[slot_g, slot_t],
            device_id=(other_g, other_t), device_id_type=LINK,
        )

    def spread(step):
        peer = lax.rem(me + step, devices)
        return peer // lanes_tp, lax.rem(peer, lanes_tp)

    def y_start(step, carry):
        a, b = spread(step)
        y_copy(a, b, g, t).start()
        return carry

    lax.fori_loop(1, devices, y_start, 0)
    y_recv[g, t] = y_send[g, t]

    def y_wait(step, carry):
        a, b = spread(step)
        y_copy(a, b, a, b).wait_recv()
        return carry

    lax.fori_loop(1, devices, y_wait, 0)
    total = res_buf[t]
    for u in range(groups):
        half = y_recv[u, 0].astype(F32)
        for i in range(1, lanes_tp):
            half = half + y_recv[u, i].astype(F32)
        weight = jnp.sum(
            jnp.where(routes[...] == u // 2, route_weights[...], 0.0), axis=1, keepdims=True
        )
        total = total + weight * half.astype(BF16).astype(F32)
    out_ref[...] = total.astype(BF16)

    for peer in peers:
        hv_copy(peer, t).wait_send()
        part_copy(peer, t).wait_send()

    def x_done(step, carry):
        a, b = others(step)
        x_copy(a, b, g, t).wait_send()
        return carry

    lax.fori_loop(0, far, x_done, 0)

    def y_done(step, carry):
        a, b = spread(step)
        y_copy(a, b, g, t).wait_send()
        return carry

    lax.fori_loop(1, devices, y_done, 0)


def fused_layer(groups, lanes_tp, *args):
    args = [a.reshape(1, -1) if a.ndim == 1 and a.dtype == F32 else a for a in args]
    spots = np.arange(HEADS * ROPE) % (ROPE // 2)
    args.append(jnp.asarray((rope_base ** (-2.0 * spots / ROPE))[None].astype(np.float32)))
    rows, width = args[0].shape
    own = args[14].shape[0]
    quarter = width // lanes_tp
    block = HEADS * VDIM // lanes_tp
    local = [
        pltpu.SMEM(a.shape, a.dtype) if i == 14 else pltpu.VMEM(a.shape, a.dtype)
        for i, a in enumerate(args)
    ]
    sem = pltpu.SemaphoreType.DMA
    return pl.pallas_call(
        functools.partial(layer_kernel, groups, lanes_tp),
        out_shape=jax.ShapeDtypeStruct((rows, quarter), BF16),
        in_specs=[pl.BlockSpec(memory_space=pl.ANY)] * len(args),
        out_specs=pl.BlockSpec(memory_space=pltpu.VMEM),
        scratch_shapes=local
        + [
            sem((len(args),)),
            pltpu.VMEM((lanes_tp, 8, block), F32),
            pltpu.VMEM((lanes_tp, 8, block), F32),
            pltpu.VMEM((rows, block), F32),
            pltpu.VMEM((lanes_tp, rows, width), BF16),
            pltpu.VMEM((lanes_tp, rows, quarter), F32),
            pltpu.VMEM((groups, lanes_tp, rows, quarter), BF16),
            pltpu.VMEM((groups, lanes_tp, rows, quarter), BF16),
            pltpu.VMEM((groups, lanes_tp, rows, quarter), BF16),
            sem((lanes_tp,)), sem((lanes_tp,)), sem((lanes_tp,)), sem((lanes_tp,)),
            sem((groups, lanes_tp)), sem((groups, lanes_tp)),
            sem((groups, lanes_tp)), sem((groups, lanes_tp)),
        ],
        compiler_params=pltpu.CompilerParams(
            collective_id=0, has_side_effects=True, vmem_limit_bytes=60 * 1024 * 1024
        ),
    )(*args)


def pick_form(groups, lanes_tp, *args):
    rows = args[0].shape[0]
    if max(2, 4 * rows // (groups // 2)) < rows:
        return per_device(*args)
    return fused_layer(groups, lanes_tp, *args)


def solution(mesh):
    placed = (
        P("ep", None),
        P(),
        P(),
        P(),
        P(),
        P(),
        P(),
        P(),
        P(),
        P(),
        P(),
        P("tp", None),
        P(("ep", "tp"), None, None),
        P(("ep", "tp"), None, None),
        P(("ep", "tp")),
        P(),
        P("ep", None),
        P("ep", None),
        P("ep", None, "tp"),
        P("ep", None, "tp"),
        P("ep", "tp", None),
    )
    step = functools.partial(pick_form, mesh.shape["ep"], mesh.shape["tp"])
    return jax.shard_map(
        step, mesh=mesh, in_specs=placed, out_specs=P("ep", "tp"), check_vma=False
    )
```

```python
import functools

import jax
import jax.numpy as jnp
import numpy as np
from jax import lax
from jax.experimental import pallas as pl
from jax.experimental.pallas import tpu as pltpu
from jax.sharding import PartitionSpec as P

HEADS = 8
NOPE = 64
ROPE = 32
VDIM = 64
KVLORA = 128


eps = 1e-06
rope_base = 10000.0


def rms_scale(values, gain):
    return values * lax.rsqrt(jnp.mean(values * values, axis=-1, keepdims=True) + eps) * gain


def rotate(values, positions):
    width = values.shape[-1]
    middle = width // 2
    inverse = jnp.power(rope_base, -jnp.arange(0, width, 2).astype(jnp.float32) / width)
    angles = positions.astype(jnp.float32)[:, None] * inverse[None, :]
    angles = jnp.concatenate([angles, angles], axis=-1)
    target = (angles.shape[0],) + (1,) * (values.ndim - 2) + (width,)
    cosine = jnp.cos(angles).reshape(target)
    sine = jnp.sin(angles).reshape(target)
    turned = jnp.concatenate([-values[..., middle:], values[..., :middle]], axis=-1)
    return values * cosine + turned * sine


def route_slots(route_table, expert_count):
    flat_ids = route_table.reshape(-1)
    onehot = (flat_ids[:, None] == jnp.arange(expert_count, dtype=jnp.int32)[None, :]).astype(
        jnp.int32
    )
    before = jnp.cumsum(onehot, axis=0) - onehot
    return jnp.sum(before * onehot, axis=1).reshape(route_table.shape)


def unit_block(arrived, w_gate, w_up, w_down):
    gate_part = jnp.einsum("scd,df->scf", arrived, w_gate[0], preferred_element_type=jnp.float32)
    up_part = jnp.einsum("scd,df->scf", arrived, w_up[0], preferred_element_type=jnp.float32)
    inner = (jax.nn.silu(gate_part) * up_part).astype(jnp.bfloat16)
    block_term = jnp.einsum("scf,fd->scd", inner, w_down[0], preferred_element_type=jnp.float32)
    summed = lax.psum_scatter(
        block_term.astype(jnp.bfloat16), "tp", scatter_dimension=2, tiled=True
    )
    return lax.all_to_all(summed, "ep", split_axis=0, concat_axis=0, tiled=True)


def per_device(
    hidden_in,
    attn_gain,
    w_qdown,
    q_gain,
    w_qnope,
    w_qrope,
    w_kvdown,
    kv_gain,
    w_krope,
    w_ukey,
    w_uvalue,
    w_out,
    cache_latent,
    cache_rope,
    lengths,
    ffn_gain,
    routes,
    route_weights,
    w_gate,
    w_up,
    w_down,
):
    group_rows, width = hidden_in.shape
    own_count = lengths.shape[0]
    tp_rank = lax.axis_index("tp")
    score_scale = (NOPE + ROPE) ** (-0.5)
    own_rows = lax.dynamic_slice_in_dim(hidden_in, tp_rank * own_count, own_count, 0).astype(
        jnp.float32
    )
    normed = rms_scale(own_rows, attn_gain).astype(jnp.bfloat16)
    q_small = rms_scale(
        jnp.dot(normed, w_qdown, preferred_element_type=jnp.float32), q_gain
    ).astype(jnp.bfloat16)
    q_plain = (
        jnp.dot(q_small, w_qnope, preferred_element_type=jnp.float32)
        .astype(jnp.bfloat16)
        .reshape(own_count, HEADS, NOPE)
    )
    q_turned = rotate(
        jnp.dot(q_small, w_qrope, preferred_element_type=jnp.float32).reshape(
            own_count, HEADS, ROPE
        ),
        lengths,
    ).astype(jnp.bfloat16)
    q_latent = jnp.einsum(
        "shn,chn->shc",
        q_plain,
        w_ukey.reshape(KVLORA, HEADS, NOPE),
        preferred_element_type=jnp.float32,
    ).astype(jnp.bfloat16)
    new_latent = rms_scale(
        jnp.dot(normed, w_kvdown, preferred_element_type=jnp.float32), kv_gain
    ).astype(jnp.bfloat16)
    new_rope = rotate(jnp.dot(normed, w_krope, preferred_element_type=jnp.float32), lengths).astype(
        jnp.bfloat16
    )
    past_scores = (
        jnp.einsum("shc,spc->shp", q_latent, cache_latent, preferred_element_type=jnp.float32)
        + jnp.einsum("shr,srp->shp", q_turned, cache_rope, preferred_element_type=jnp.float32)
    ) * score_scale
    in_range = jnp.arange(cache_latent.shape[1])[None, None, :] < lengths[:, None, None]
    past_scores = jnp.where(in_range, past_scores, -1e30)
    fresh_score = (
        jnp.einsum("shc,sc->sh", q_latent, new_latent, preferred_element_type=jnp.float32)
        + jnp.einsum("shr,sr->sh", q_turned, new_rope, preferred_element_type=jnp.float32)
    ) * score_scale
    highest = jnp.maximum(jnp.max(past_scores, axis=-1), fresh_score)
    past_exp = jnp.exp(past_scores - highest[..., None])
    fresh_exp = jnp.exp(fresh_score - highest)
    divisor = jnp.sum(past_exp, axis=-1) + fresh_exp
    past_prob = (past_exp / divisor[..., None]).astype(jnp.bfloat16)
    fresh_prob = (fresh_exp / divisor).astype(jnp.bfloat16)
    latent_mix = (
        jnp.einsum("shp,spc->shc", past_prob, cache_latent, preferred_element_type=jnp.float32)
        + fresh_prob.astype(jnp.float32)[..., None] * new_latent.astype(jnp.float32)[:, None, :]
    ).astype(jnp.bfloat16)
    head_values = (
        jnp.einsum(
            "shc,chv->shv",
            latent_mix,
            w_uvalue.reshape(KVLORA, HEADS, VDIM),
            preferred_element_type=jnp.float32,
        )
        .astype(jnp.bfloat16)
        .reshape(own_count, HEADS * VDIM)
    )
    by_heads = lax.all_to_all(head_values, "tp", split_axis=1, concat_axis=0, tiled=True)
    attended = lax.psum(
        jnp.dot(by_heads, w_out, preferred_element_type=jnp.float32).astype(jnp.bfloat16), "tp"
    ).astype(jnp.float32)
    residual = hidden_in.astype(jnp.float32) + attended
    normed_two = rms_scale(residual, ffn_gain).astype(jnp.bfloat16)
    unit_count = lax.axis_size("ep")
    expert_count = unit_count // 2
    capacity = max(2, 4 * group_rows // expert_count)
    quarter = width // lax.axis_size("tp")
    slots = route_slots(routes, expert_count)
    expert_of_unit = jnp.arange(unit_count, dtype=jnp.int32) // 2
    slot_range = jnp.arange(capacity, dtype=jnp.int32)
    chosen = (routes[None, None, :, :] == expert_of_unit[:, None, None, None]) & (
        slots[None, None, :, :] == slot_range[None, :, None, None]
    )
    chooser = jnp.sum(chosen.astype(jnp.int32), axis=-1).astype(jnp.bfloat16)
    outgoing = jnp.einsum(
        "ucr,rd->ucd", chooser, normed_two, preferred_element_type=jnp.float32
    ).astype(jnp.bfloat16)
    returned = unit_block(
        lax.all_to_all(outgoing, "ep", split_axis=0, concat_axis=0, tiled=True),
        w_gate,
        w_up,
        w_down,
    )
    stacked = returned.reshape(unit_count * capacity, quarter)
    first_row = routes * (2 * capacity) + slots
    first_half = stacked[first_row].astype(jnp.float32)
    second_half = stacked[first_row + capacity].astype(jnp.float32)
    blended = jnp.sum(route_weights[..., None] * (first_half + second_half), axis=1)
    own_columns = lax.dynamic_slice_in_dim(residual, tp_rank * quarter, quarter, 1)
    return (own_columns + blended).astype(jnp.bfloat16)


LINK = pl.DeviceIdType.MESH
F32 = jnp.float32
BF16 = jnp.bfloat16


def mm(a, b):
    return jnp.dot(a, b, preferred_element_type=F32)


def mm_nt(a, b):
    return lax.dot_general(a, b, (((1,), (1,)), ((), ())), preferred_element_type=F32)


def iota(shape, dim):
    return lax.broadcasted_iota(jnp.int32, shape, dim)


def layer_kernel(groups, lanes_tp, *refs):
    names = 22
    hbm, out_ref = refs[:names], refs[names]
    local = refs[names + 1 : 2 * names + 1]
    (
        load_sem, hv_send, hv_recv, rows_buf, part, res_buf, x_buf, y_send, y_recv,
        hv_ss, hv_rs, part_ss, part_rs, x_ss, x_rs, y_ss, y_rs,
    ) = refs[2 * names + 1 :]
    (
        hidden, attn_gain, w_qdown, q_gain, w_qnope, w_qrope, w_kvdown, kv_gain, w_krope,
        w_ukey, w_uvalue, w_out, cache_latent, cache_rope, lengths, ffn_gain, routes,
        route_weights, w_gate, w_up, w_down, inverse,
    ) = local
    g, t = lax.axis_index("ep"), lax.axis_index("tp")
    devices = groups * lanes_tp
    me = g * lanes_tp + t

    barrier = pltpu.get_barrier_semaphore()

    def greet(step, carry):
        peer = lax.rem(me + step, devices)
        pl.semaphore_signal(
            barrier, inc=1, device_id=(peer // lanes_tp, lax.rem(peer, lanes_tp)),
            device_id_type=LINK,
        )
        return carry

    lax.fori_loop(1, devices, greet, 0)

    loads = [
        pltpu.make_async_copy(hbm[i], local[i], load_sem.at[i]) for i in range(names)
    ]
    order = [0, 1, 2, 3, 14, 21, 6, 8, 7, 4, 5, 9, 12, 13, 10, 11, 15, 16, 17, 18, 19, 20]
    for i in order:
        loads[i].start()

    own = lengths.shape[0]
    rows, width = hidden.shape
    quarter = width // lanes_tp
    pad = 8

    for i in (0, 1, 2, 3):
        loads[i].wait()
    pick = (iota((pad, rows), 1) == iota((pad, rows), 0) + t * own) & (
        iota((pad, rows), 0) < own
    )
    mine = mm(jnp.where(pick, 1.0, 0.0).astype(BF16), hidden[...])
    normed = rms_scale(mine, attn_gain[...]).astype(BF16)
    q_small = rms_scale(mm(normed, w_qdown[...]), q_gain[...]).astype(BF16)
    for i in (14, 21, 6, 8, 7, 4, 5):
        loads[i].wait()
    position = jnp.zeros((pad, 1), jnp.int32)
    for s in range(own):
        position = jnp.where(iota((pad, 1), 0) == s, lengths[s], position)
    angles = position.astype(F32) * inverse[...]
    cosine, sine = jnp.cos(angles), jnp.sin(angles)
    new_latent = rms_scale(mm(normed, w_kvdown[...]), kv_gain[...]).astype(BF16).astype(F32)
    rope_key = mm_nt(normed, w_krope[...])
    turned_key = jnp.concatenate([-rope_key[:, ROPE // 2 :], rope_key[:, : ROPE // 2]], axis=1)
    new_rope = rope_key * cosine[:, :ROPE] + turned_key * sine[:, :ROPE]
    new_rope = new_rope.astype(BF16).astype(F32)
    q_plain = mm(q_small, w_qnope[...]).astype(BF16).astype(F32)
    q_rope = mm(q_small, w_qrope[...])
    span = HEADS * ROPE
    first = (iota((pad, span), 1) & (ROPE - 1)) < ROPE // 2
    turned = jnp.where(
        first, -pltpu.roll(q_rope, span - ROPE // 2, 1), pltpu.roll(q_rope, ROPE // 2, 1)
    )
    q_turned = (q_rope * cosine + turned * sine).astype(BF16).astype(F32)
    plain_mask = iota((HEADS, HEADS * NOPE), 1) // NOPE == iota((HEADS, HEADS * NOPE), 0)
    rope_mask = iota((HEADS, span), 1) // ROPE == iota((HEADS, span), 0)
    plain_rows = jnp.concatenate(
        [jnp.where(plain_mask, q_plain[s : s + 1, :], 0.0) for s in range(own)], axis=0
    ).astype(BF16)
    rope_rows = jnp.concatenate(
        [jnp.where(rope_mask, q_turned[s : s + 1, :], 0.0) for s in range(own)], axis=0
    ).astype(BF16)
    fold = ((iota((span, ROPE), 0) & (ROPE - 1)) == iota((span, ROPE), 1)).astype(F32)
    q_heads = mm(rope_rows, fold.astype(BF16))
    loads[9].wait()
    q_latent = mm_nt(plain_rows, w_ukey[...]).astype(BF16)
    loads[12].wait()
    loads[13].wait()
    scale = (NOPE + ROPE) ** (-0.5)
    cache = cache_latent.shape[1]
    mixes = []
    for s in range(own):
        heads = slice(s * HEADS, (s + 1) * HEADS)
        ql, qr = q_latent[heads], q_heads[heads]
        scores = (mm_nt(ql, cache_latent[s]) + mm(qr.astype(BF16), cache_rope[s])) * scale
        scores = jnp.where(iota((HEADS, cache), 1) < lengths[s], scores, -1e30)
        fresh = (
            jnp.sum(ql.astype(F32) * new_latent[s : s + 1, :], axis=1, keepdims=True)
            + jnp.sum(qr * new_rope[s : s + 1, :], axis=1, keepdims=True)
        ) * scale
        highest = jnp.maximum(jnp.max(scores, axis=1, keepdims=True), fresh)
        past_exp = jnp.exp(scores - highest)
        fresh_exp = jnp.exp(fresh - highest)
        divisor = jnp.sum(past_exp, axis=1, keepdims=True) + fresh_exp
        past_prob = (past_exp / divisor).astype(BF16)
        fresh_prob = (fresh_exp / divisor).astype(BF16).astype(F32)
        mixes.append(mm(past_prob, cache_latent[s]) + fresh_prob * new_latent[s : s + 1, :])
    loads[10].wait()
    mix = jnp.concatenate(mixes, axis=0).astype(BF16)
    values = mm(mix, w_uvalue[...])
    value_mask = iota((HEADS, HEADS * VDIM), 1) // VDIM == iota((HEADS, HEADS * VDIM), 0)
    block = HEADS * VDIM // lanes_tp
    for s in range(own):
        row = jnp.sum(
            jnp.where(value_mask, values[s * HEADS : (s + 1) * HEADS], 0.0), axis=0, keepdims=True
        )
        row = row.astype(BF16).astype(F32)
        for i in range(lanes_tp):
            hv_send[i, s : s + 1, :] = row[:, i * block : (i + 1) * block]

    pl.semaphore_wait(barrier, devices - 1)

    def hv_copy(peer, slot):
        return pltpu.make_async_remote_copy(
            hv_send.at[peer], hv_recv.at[slot], hv_ss.at[peer], hv_rs.at[slot],
            device_id=(g, peer), device_id_type=LINK,
        )

    peers = [lax.rem(t + i, lanes_tp) for i in range(1, lanes_tp)]
    for peer in peers:
        hv_copy(peer, t).start()
    hv_recv[t] = hv_send[t]
    loads[11].wait()
    loads[15].wait()
    for peer in peers:
        hv_copy(peer, peer).wait_recv()
    for i in range(lanes_tp):
        rows_buf[i * own : (i + 1) * own, :] = hv_recv[i, :own, :]
    part[t] = mm(rows_buf[...].astype(BF16), w_out[...]).astype(BF16)

    def part_copy(peer, slot):
        return pltpu.make_async_remote_copy(
            part.at[slot], part.at[slot], part_ss.at[peer], part_rs.at[slot],
            device_id=(g, peer), device_id_type=LINK,
        )

    for peer in peers:
        part_copy(peer, t).start()
    for peer in peers:
        part_copy(peer, peer).wait_recv()
    attended = part[0].astype(F32)
    for i in range(1, lanes_tp):
        attended = attended + part[i].astype(F32)
    residual = hidden[...].astype(F32) + attended
    normed_two = rms_scale(residual, ffn_gain[...]).astype(BF16)
    for i in range(lanes_tp):
        x_buf[g, i] = normed_two[:, i * quarter : (i + 1) * quarter]
        res_buf[i] = residual[:, i * quarter : (i + 1) * quarter]

    def x_copy(other_g, other_t, slot_g, slot_t):
        return pltpu.make_async_remote_copy(
            x_buf.at[slot_g, slot_t], x_buf.at[slot_g, slot_t],
            x_ss.at[other_g, other_t], x_rs.at[slot_g, slot_t],
            device_id=(other_g, other_t), device_id_type=LINK,
        )

    def others(step):
        return lax.rem(g + 1 + step // lanes_tp, groups), lax.rem(t + step, lanes_tp)

    far = (groups - 1) * lanes_tp

    def x_start(step, carry):
        a, b = others(step)
        x_copy(a, b, g, t).start()
        return carry

    lax.fori_loop(0, far, x_start, 0)
    for i in (16, 17, 18, 19, 20):
        loads[i].wait()

    def x_wait(step, carry):
        a, b = others(step)
        x_copy(a, b, a, b).wait_recv()
        return carry

    lax.fori_loop(0, far, x_wait, 0)

    tokens = groups * rows
    gate = jnp.zeros((tokens, w_gate.shape[1]), F32)
    up = jnp.zeros((tokens, w_gate.shape[1]), F32)
    for i in range(lanes_tp):
        piece = x_buf[:, i].reshape(tokens, quarter)
        depth = slice(i * quarter, (i + 1) * quarter)
        gate = gate + mm_nt(piece, w_gate[0, :, depth])
        up = up + mm_nt(piece, w_up[0, :, depth])
    inner = (gate / (1.0 + jnp.exp(-gate)) * up).astype(BF16)
    for i in range(lanes_tp):
        term = mm(inner, w_down[0, :, i * quarter : (i + 1) * quarter]).astype(BF16)
        y_send[:, i] = term.reshape(groups, rows, quarter)

    same = iota((rows, rows), 0) == iota((rows, rows), 1)
    weights = []
    for e in range(groups // 2):
        flat = jnp.sum(
            jnp.where(routes[...] == e, route_weights[...], 0.0), axis=0, keepdims=True
        )
        weights.append(jnp.sum(jnp.where(same, flat, 0.0), axis=1, keepdims=True))

    def y_copy(other_g, other_t, slot_g, slot_t):
        return pltpu.make_async_remote_copy(
            y_send.at[other_g, other_t], y_recv.at[slot_g, slot_t],
            y_ss.at[other_g, other_t], y_rs.at[slot_g, slot_t],
            device_id=(other_g, other_t), device_id_type=LINK,
        )

    def spread(step):
        peer = lax.rem(me + step, devices)
        return peer // lanes_tp, lax.rem(peer, lanes_tp)

    def y_start(step, carry):
        a, b = spread(step)
        y_copy(a, b, g, t).start()
        return carry

    lax.fori_loop(1, devices, y_start, 0)
    y_recv[g, t] = y_send[g, t]

    def y_wait(step, carry):
        a, b = spread(step)
        y_copy(a, b, a, b).wait_recv()
        return carry

    lax.fori_loop(1, devices, y_wait, 0)
    total = res_buf[t]
    for u in range(groups):
        half = y_recv[u, 0].astype(F32)
        for i in range(1, lanes_tp):
            half = half + y_recv[u, i].astype(F32)
        total = total + weights[u // 2] * half.astype(BF16).astype(F32)
    out_ref[...] = total

    for peer in peers:
        hv_copy(peer, t).wait_send()
        part_copy(peer, t).wait_send()

    def x_done(step, carry):
        a, b = others(step)
        x_copy(a, b, g, t).wait_send()
        return carry

    lax.fori_loop(0, far, x_done, 0)

    def y_done(step, carry):
        a, b = spread(step)
        y_copy(a, b, g, t).wait_send()
        return carry

    lax.fori_loop(1, devices, y_done, 0)


def fused_layer(groups, lanes_tp, *args):
    args = list(args)
    for i in (8, 16, 17):
        args[i] = args[i].T
    for i in (18, 19):
        args[i] = args[i].swapaxes(1, 2)
    args = [a.reshape(1, -1) if a.ndim == 1 and a.dtype == F32 else a for a in args]
    spots = np.arange(HEADS * ROPE) % (ROPE // 2)
    args.append(jnp.asarray((rope_base ** (-2.0 * spots / ROPE))[None].astype(np.float32)))
    rows, width = args[0].shape
    own = args[14].shape[0]
    quarter = width // lanes_tp
    block = HEADS * VDIM // lanes_tp
    local = [
        pltpu.SMEM(a.shape, a.dtype) if i == 14 else pltpu.VMEM(a.shape, a.dtype)
        for i, a in enumerate(args)
    ]
    sem = pltpu.SemaphoreType.DMA
    return pl.pallas_call(
        functools.partial(layer_kernel, groups, lanes_tp),
        out_shape=jax.ShapeDtypeStruct((rows, quarter), F32),
        in_specs=[pl.BlockSpec(memory_space=pl.ANY)] * len(args),
        out_specs=pl.BlockSpec(memory_space=pltpu.VMEM),
        scratch_shapes=local
        + [
            sem((len(args),)),
            pltpu.VMEM((lanes_tp, 8, block), F32),
            pltpu.VMEM((lanes_tp, 8, block), F32),
            pltpu.VMEM((rows, block), F32),
            pltpu.VMEM((lanes_tp, rows, width), BF16),
            pltpu.VMEM((lanes_tp, rows, quarter), F32),
            pltpu.VMEM((groups, lanes_tp, rows, quarter), BF16),
            pltpu.VMEM((groups, lanes_tp, rows, quarter), BF16),
            pltpu.VMEM((groups, lanes_tp, rows, quarter), BF16),
            sem((lanes_tp,)), sem((lanes_tp,)), sem((lanes_tp,)), sem((lanes_tp,)),
            sem((groups, lanes_tp)), sem((groups, lanes_tp)),
            sem((groups, lanes_tp)), sem((groups, lanes_tp)),
        ],
        compiler_params=pltpu.CompilerParams(
            collective_id=0, has_side_effects=True, vmem_limit_bytes=60 * 1024 * 1024
        ),
    )(*args).astype(BF16)


def pick_form(groups, lanes_tp, *args):
    rows = args[0].shape[0]
    if max(2, 4 * rows // (groups // 2)) < rows:
        return per_device(*args)
    return fused_layer(groups, lanes_tp, *args)


def solution(mesh):
    placed = (
        P("ep", None),
        P(),
        P(),
        P(),
        P(),
        P(),
        P(),
        P(),
        P(),
        P(),
        P(),
        P("tp", None),
        P(("ep", "tp"), None, None),
        P(("ep", "tp"), None, None),
        P(("ep", "tp")),
        P(),
        P("ep", None),
        P("ep", None),
        P("ep", None, "tp"),
        P("ep", None, "tp"),
        P("ep", "tp", None),
    )
    step = functools.partial(pick_form, mesh.shape["ep"], mesh.shape["tp"])
    return jax.shard_map(
        step, mesh=mesh, in_specs=placed, out_specs=P("ep", "tp"), check_vma=False
    )
```

```python
import functools

import jax
import jax.numpy as jnp
import numpy as np
from jax import lax
from jax.experimental import pallas as pl
from jax.experimental.pallas import tpu as pltpu
from jax.sharding import PartitionSpec as P

HEADS = 8
NOPE = 64
ROPE = 32
VDIM = 64
KVLORA = 128


eps = 1e-06
rope_base = 10000.0


def rms_scale(values, gain):
    return values * lax.rsqrt(jnp.mean(values * values, axis=-1, keepdims=True) + eps) * gain


def rotate(values, positions):
    width = values.shape[-1]
    middle = width // 2
    inverse = jnp.power(rope_base, -jnp.arange(0, width, 2).astype(jnp.float32) / width)
    angles = positions.astype(jnp.float32)[:, None] * inverse[None, :]
    angles = jnp.concatenate([angles, angles], axis=-1)
    target = (angles.shape[0],) + (1,) * (values.ndim - 2) + (width,)
    cosine = jnp.cos(angles).reshape(target)
    sine = jnp.sin(angles).reshape(target)
    turned = jnp.concatenate([-values[..., middle:], values[..., :middle]], axis=-1)
    return values * cosine + turned * sine


def route_slots(route_table, expert_count):
    flat_ids = route_table.reshape(-1)
    onehot = (flat_ids[:, None] == jnp.arange(expert_count, dtype=jnp.int32)[None, :]).astype(
        jnp.int32
    )
    before = jnp.cumsum(onehot, axis=0) - onehot
    return jnp.sum(before * onehot, axis=1).reshape(route_table.shape)


def unit_block(arrived, w_gate, w_up, w_down):
    gate_part = jnp.einsum("scd,df->scf", arrived, w_gate[0], preferred_element_type=jnp.float32)
    up_part = jnp.einsum("scd,df->scf", arrived, w_up[0], preferred_element_type=jnp.float32)
    inner = (jax.nn.silu(gate_part) * up_part).astype(jnp.bfloat16)
    block_term = jnp.einsum("scf,fd->scd", inner, w_down[0], preferred_element_type=jnp.float32)
    summed = lax.psum_scatter(
        block_term.astype(jnp.bfloat16), "tp", scatter_dimension=2, tiled=True
    )
    return lax.all_to_all(summed, "ep", split_axis=0, concat_axis=0, tiled=True)


def per_device(
    hidden_in,
    attn_gain,
    w_qdown,
    q_gain,
    w_qnope,
    w_qrope,
    w_kvdown,
    kv_gain,
    w_krope,
    w_ukey,
    w_uvalue,
    w_out,
    cache_latent,
    cache_rope,
    lengths,
    ffn_gain,
    routes,
    route_weights,
    w_gate,
    w_up,
    w_down,
):
    group_rows, width = hidden_in.shape
    own_count = lengths.shape[0]
    tp_rank = lax.axis_index("tp")
    score_scale = (NOPE + ROPE) ** (-0.5)
    own_rows = lax.dynamic_slice_in_dim(hidden_in, tp_rank * own_count, own_count, 0).astype(
        jnp.float32
    )
    normed = rms_scale(own_rows, attn_gain).astype(jnp.bfloat16)
    q_small = rms_scale(
        jnp.dot(normed, w_qdown, preferred_element_type=jnp.float32), q_gain
    ).astype(jnp.bfloat16)
    q_plain = (
        jnp.dot(q_small, w_qnope, preferred_element_type=jnp.float32)
        .astype(jnp.bfloat16)
        .reshape(own_count, HEADS, NOPE)
    )
    q_turned = rotate(
        jnp.dot(q_small, w_qrope, preferred_element_type=jnp.float32).reshape(
            own_count, HEADS, ROPE
        ),
        lengths,
    ).astype(jnp.bfloat16)
    q_latent = jnp.einsum(
        "shn,chn->shc",
        q_plain,
        w_ukey.reshape(KVLORA, HEADS, NOPE),
        preferred_element_type=jnp.float32,
    ).astype(jnp.bfloat16)
    new_latent = rms_scale(
        jnp.dot(normed, w_kvdown, preferred_element_type=jnp.float32), kv_gain
    ).astype(jnp.bfloat16)
    new_rope = rotate(jnp.dot(normed, w_krope, preferred_element_type=jnp.float32), lengths).astype(
        jnp.bfloat16
    )
    past_scores = (
        jnp.einsum("shc,spc->shp", q_latent, cache_latent, preferred_element_type=jnp.float32)
        + jnp.einsum("shr,srp->shp", q_turned, cache_rope, preferred_element_type=jnp.float32)
    ) * score_scale
    in_range = jnp.arange(cache_latent.shape[1])[None, None, :] < lengths[:, None, None]
    past_scores = jnp.where(in_range, past_scores, -1e30)
    fresh_score = (
        jnp.einsum("shc,sc->sh", q_latent, new_latent, preferred_element_type=jnp.float32)
        + jnp.einsum("shr,sr->sh", q_turned, new_rope, preferred_element_type=jnp.float32)
    ) * score_scale
    highest = jnp.maximum(jnp.max(past_scores, axis=-1), fresh_score)
    past_exp = jnp.exp(past_scores - highest[..., None])
    fresh_exp = jnp.exp(fresh_score - highest)
    divisor = jnp.sum(past_exp, axis=-1) + fresh_exp
    past_prob = (past_exp / divisor[..., None]).astype(jnp.bfloat16)
    fresh_prob = (fresh_exp / divisor).astype(jnp.bfloat16)
    latent_mix = (
        jnp.einsum("shp,spc->shc", past_prob, cache_latent, preferred_element_type=jnp.float32)
        + fresh_prob.astype(jnp.float32)[..., None] * new_latent.astype(jnp.float32)[:, None, :]
    ).astype(jnp.bfloat16)
    head_values = (
        jnp.einsum(
            "shc,chv->shv",
            latent_mix,
            w_uvalue.reshape(KVLORA, HEADS, VDIM),
            preferred_element_type=jnp.float32,
        )
        .astype(jnp.bfloat16)
        .reshape(own_count, HEADS * VDIM)
    )
    by_heads = lax.all_to_all(head_values, "tp", split_axis=1, concat_axis=0, tiled=True)
    attended = lax.psum(
        jnp.dot(by_heads, w_out, preferred_element_type=jnp.float32).astype(jnp.bfloat16), "tp"
    ).astype(jnp.float32)
    residual = hidden_in.astype(jnp.float32) + attended
    normed_two = rms_scale(residual, ffn_gain).astype(jnp.bfloat16)
    unit_count = lax.axis_size("ep")
    expert_count = unit_count // 2
    capacity = max(2, 4 * group_rows // expert_count)
    quarter = width // lax.axis_size("tp")
    slots = route_slots(routes, expert_count)
    expert_of_unit = jnp.arange(unit_count, dtype=jnp.int32) // 2
    slot_range = jnp.arange(capacity, dtype=jnp.int32)
    chosen = (routes[None, None, :, :] == expert_of_unit[:, None, None, None]) & (
        slots[None, None, :, :] == slot_range[None, :, None, None]
    )
    chooser = jnp.sum(chosen.astype(jnp.int32), axis=-1).astype(jnp.bfloat16)
    outgoing = jnp.einsum(
        "ucr,rd->ucd", chooser, normed_two, preferred_element_type=jnp.float32
    ).astype(jnp.bfloat16)
    returned = unit_block(
        lax.all_to_all(outgoing, "ep", split_axis=0, concat_axis=0, tiled=True),
        w_gate,
        w_up,
        w_down,
    )
    stacked = returned.reshape(unit_count * capacity, quarter)
    first_row = routes * (2 * capacity) + slots
    first_half = stacked[first_row].astype(jnp.float32)
    second_half = stacked[first_row + capacity].astype(jnp.float32)
    blended = jnp.sum(route_weights[..., None] * (first_half + second_half), axis=1)
    own_columns = lax.dynamic_slice_in_dim(residual, tp_rank * quarter, quarter, 1)
    return (own_columns + blended).astype(jnp.bfloat16)


LINK = pl.DeviceIdType.MESH
F32 = jnp.float32
BF16 = jnp.bfloat16


def mm(a, b):
    return jnp.dot(a, b, preferred_element_type=F32)


def mm_nt(a, b):
    return lax.dot_general(a, b, (((1,), (1,)), ((), ())), preferred_element_type=F32)


def iota(shape, dim):
    return lax.broadcasted_iota(jnp.int32, shape, dim)


def layer_kernel(groups, lanes_tp, *refs):
    names = 22
    hbm, out_ref = refs[:names], refs[names]
    local = refs[names + 1 : 2 * names + 1]
    (
        load_sem, hv_send, hv_recv, rows_buf, part, res_buf, x_buf, y_send, y_recv,
        hv_ss, hv_rs, part_ss, part_rs, x_ss, x_rs, f_ss, f_rs, y_ss, y_rs,
    ) = refs[2 * names + 1 :]
    (
        hidden, attn_gain, w_qdown, q_gain, w_qnope, w_qrope, w_kvdown, kv_gain, w_krope,
        w_ukey, w_uvalue, w_out, cache_latent, cache_rope, lengths, ffn_gain, routes,
        route_weights, w_gate, w_up, w_down, inverse,
    ) = local
    g, t = lax.axis_index("ep"), lax.axis_index("tp")
    devices = groups * lanes_tp
    me = g * lanes_tp + t

    barrier = pltpu.get_barrier_semaphore()

    def ring(step):
        return lax.rem(g + step, groups)

    peers = [lax.rem(t + i, lanes_tp) for i in range(1, lanes_tp)]
    for peer in peers:
        pl.semaphore_signal(barrier, inc=1, device_id=(g, peer), device_id_type=LINK)
    for i in range(1, groups):
        pl.semaphore_signal(barrier, inc=1, device_id=(ring(i), t), device_id_type=LINK)

    loads = [
        pltpu.make_async_copy(hbm[i], local[i], load_sem.at[i]) for i in range(names)
    ]
    order = [0, 1, 2, 3, 14, 21, 6, 8, 7, 4, 5, 9, 12, 13, 10, 11, 15, 16, 17, 18, 19, 20]
    for i in order:
        loads[i].start()

    own = lengths.shape[0]
    rows, width = hidden.shape
    quarter = width // lanes_tp
    pad = 8

    for i in (0, 1, 2, 3):
        loads[i].wait()
    pick = (iota((pad, rows), 1) == iota((pad, rows), 0) + t * own) & (
        iota((pad, rows), 0) < own
    )
    mine = mm(jnp.where(pick, 1.0, 0.0).astype(BF16), hidden[...])
    normed = rms_scale(mine, attn_gain[...]).astype(BF16)
    q_small = rms_scale(mm(normed, w_qdown[...]), q_gain[...]).astype(BF16)
    for i in (14, 21, 6, 8, 7, 4, 5):
        loads[i].wait()
    position = jnp.zeros((pad, 1), jnp.int32)
    for s in range(own):
        position = jnp.where(iota((pad, 1), 0) == s, lengths[s], position)
    angles = position.astype(F32) * inverse[...]
    cosine, sine = jnp.cos(angles), jnp.sin(angles)
    new_latent = rms_scale(mm(normed, w_kvdown[...]), kv_gain[...]).astype(BF16).astype(F32)
    rope_key = mm_nt(normed, w_krope[...])
    turned_key = jnp.concatenate([-rope_key[:, ROPE // 2 :], rope_key[:, : ROPE // 2]], axis=1)
    new_rope = rope_key * cosine[:, :ROPE] + turned_key * sine[:, :ROPE]
    new_rope = new_rope.astype(BF16).astype(F32)
    q_plain = mm(q_small, w_qnope[...]).astype(BF16).astype(F32)
    q_rope = mm(q_small, w_qrope[...])
    span = HEADS * ROPE
    first = (iota((pad, span), 1) & (ROPE - 1)) < ROPE // 2
    turned = jnp.where(
        first, -pltpu.roll(q_rope, span - ROPE // 2, 1), pltpu.roll(q_rope, ROPE // 2, 1)
    )
    q_turned = (q_rope * cosine + turned * sine).astype(BF16).astype(F32)
    plain_mask = iota((HEADS, HEADS * NOPE), 1) // NOPE == iota((HEADS, HEADS * NOPE), 0)
    rope_mask = iota((HEADS, span), 1) // ROPE == iota((HEADS, span), 0)
    plain_rows = jnp.concatenate(
        [jnp.where(plain_mask, q_plain[s : s + 1, :], 0.0) for s in range(own)], axis=0
    ).astype(BF16)
    rope_rows = jnp.concatenate(
        [jnp.where(rope_mask, q_turned[s : s + 1, :], 0.0) for s in range(own)], axis=0
    ).astype(BF16)
    fold = ((iota((span, ROPE), 0) & (ROPE - 1)) == iota((span, ROPE), 1)).astype(F32)
    q_heads = mm(rope_rows, fold.astype(BF16))
    loads[9].wait()
    q_latent = mm_nt(plain_rows, w_ukey[...]).astype(BF16)
    loads[12].wait()
    loads[13].wait()
    scale = (NOPE + ROPE) ** (-0.5)
    cache = cache_latent.shape[1]
    mixes = []
    for s in range(own):
        heads = slice(s * HEADS, (s + 1) * HEADS)
        ql, qr = q_latent[heads], q_heads[heads]
        scores = (mm_nt(ql, cache_latent[s]) + mm(qr.astype(BF16), cache_rope[s])) * scale
        scores = jnp.where(iota((HEADS, cache), 1) < lengths[s], scores, -1e30)
        fresh = (
            jnp.sum(ql.astype(F32) * new_latent[s : s + 1, :], axis=1, keepdims=True)
            + jnp.sum(qr * new_rope[s : s + 1, :], axis=1, keepdims=True)
        ) * scale
        highest = jnp.maximum(jnp.max(scores, axis=1, keepdims=True), fresh)
        past_exp = jnp.exp(scores - highest)
        fresh_exp = jnp.exp(fresh - highest)
        divisor = jnp.sum(past_exp, axis=1, keepdims=True) + fresh_exp
        past_prob = (past_exp / divisor).astype(BF16)
        fresh_prob = (fresh_exp / divisor).astype(BF16).astype(F32)
        mixes.append(mm(past_prob, cache_latent[s]) + fresh_prob * new_latent[s : s + 1, :])
    loads[10].wait()
    mix = jnp.concatenate(mixes, axis=0).astype(BF16)
    values = mm(mix, w_uvalue[...])
    value_mask = iota((HEADS, HEADS * VDIM), 1) // VDIM == iota((HEADS, HEADS * VDIM), 0)
    block = HEADS * VDIM // lanes_tp
    for s in range(own):
        row = jnp.sum(
            jnp.where(value_mask, values[s * HEADS : (s + 1) * HEADS], 0.0), axis=0, keepdims=True
        )
        row = row.astype(BF16).astype(F32)
        for i in range(lanes_tp):
            hv_send[i, s : s + 1, :] = row[:, i * block : (i + 1) * block]

    pl.semaphore_wait(barrier, groups + lanes_tp - 2)

    def hv_copy(peer, slot):
        return pltpu.make_async_remote_copy(
            hv_send.at[peer], hv_recv.at[slot], hv_ss.at[peer], hv_rs.at[slot],
            device_id=(g, peer), device_id_type=LINK,
        )

    for peer in peers:
        hv_copy(peer, t).start()
    hv_recv[t] = hv_send[t]
    loads[11].wait()
    loads[15].wait()
    for peer in peers:
        hv_copy(peer, peer).wait_recv()
    for i in range(lanes_tp):
        rows_buf[i * own : (i + 1) * own, :] = hv_recv[i, :own, :]
    part[t] = mm(rows_buf[...].astype(BF16), w_out[...]).astype(BF16)

    def part_copy(peer, slot):
        return pltpu.make_async_remote_copy(
            part.at[slot], part.at[slot], part_ss.at[peer], part_rs.at[slot],
            device_id=(g, peer), device_id_type=LINK,
        )

    for peer in peers:
        part_copy(peer, t).start()
    for peer in peers:
        part_copy(peer, peer).wait_recv()
    attended = part[0].astype(F32)
    for i in range(1, lanes_tp):
        attended = attended + part[i].astype(F32)
    residual = hidden[...].astype(F32) + attended
    normed_two = rms_scale(residual, ffn_gain[...]).astype(BF16)
    for i in range(lanes_tp):
        res_buf[i] = residual[:, i * quarter : (i + 1) * quarter]

    half_width = width // 2
    for i in range(2):
        x_buf[g, i] = normed_two[:, i * half_width : (i + 1) * half_width]

    mine_half = lax.rem(t, 2)
    partner = t + 1 - 2 * mine_half

    def x_copy(other, slot):
        return pltpu.make_async_remote_copy(
            x_buf.at[slot, mine_half], x_buf.at[slot, mine_half], x_ss.at[other], x_rs.at[slot],
            device_id=(other, t), device_id_type=LINK,
        )

    def f_copy(slot, half):
        return pltpu.make_async_remote_copy(
            x_buf.at[slot, half], x_buf.at[slot, half], f_ss.at[slot], f_rs.at[slot],
            device_id=(g, partner), device_id_type=LINK,
        )

    near = sorted(range(1, groups), key=lambda i: min(i, groups - i))
    for i in near[::-1]:
        x_copy(ring(i), g).start()
    for i in (16, 17, 18, 19, 20):
        loads[i].wait()
    for i in near:
        x_copy(ring(i), ring(i)).wait_recv()
        f_copy(ring(i), mine_half).start()
    for i in near:
        f_copy(ring(i), 1 - mine_half).wait_recv()

    def x_sends_done():
        for i in near:
            x_copy(ring(i), g).wait_send()
            f_copy(ring(i), mine_half).wait_send()

    tokens = groups * rows
    gate = jnp.zeros((tokens, w_gate.shape[1]), F32)
    up = jnp.zeros((tokens, w_gate.shape[1]), F32)
    for i in range(2):
        piece = x_buf[:, i].reshape(tokens, half_width)
        depth = slice(i * half_width, (i + 1) * half_width)
        gate = gate + mm_nt(piece, w_gate[0, :, depth])
        up = up + mm_nt(piece, w_up[0, :, depth])
    inner = (gate / (1.0 + jnp.exp(-gate)) * up).astype(BF16)
    for i in range(lanes_tp):
        term = mm(inner, w_down[0, :, i * quarter : (i + 1) * quarter]).astype(BF16)
        y_send[:, i] = term.reshape(groups, rows, quarter)

    same = iota((rows, rows), 0) == iota((rows, rows), 1)
    weights = []
    for e in range(groups // 2):
        flat = jnp.sum(
            jnp.where(routes[...] == e, route_weights[...], 0.0), axis=0, keepdims=True
        )
        weights.append(jnp.sum(jnp.where(same, flat, 0.0), axis=1, keepdims=True))

    def y_copy(other_g, other_t, slot_g, slot_t):
        return pltpu.make_async_remote_copy(
            y_send.at[other_g, other_t], y_recv.at[slot_g, slot_t],
            y_ss.at[other_g, other_t], y_rs.at[slot_g, slot_t],
            device_id=(other_g, other_t), device_id_type=LINK,
        )

    def spread(step):
        peer = lax.rem(me + step, devices)
        return peer // lanes_tp, lax.rem(peer, lanes_tp)

    def y_start(step, carry):
        a, b = spread(step)
        y_copy(a, b, g, t).start()
        return carry

    lax.fori_loop(1, devices, y_start, 0)
    y_recv[g, t] = y_send[g, t]

    def y_wait(step, carry):
        a, b = spread(step)
        y_copy(a, b, a, b).wait_recv()
        return carry

    lax.fori_loop(1, devices, y_wait, 0)
    total = res_buf[t]
    for u in range(groups):
        half = y_recv[u, 0].astype(F32)
        for i in range(1, lanes_tp):
            half = half + y_recv[u, i].astype(F32)
        total = total + weights[u // 2] * half.astype(BF16).astype(F32)
    out_ref[...] = total

    for peer in peers:
        hv_copy(peer, t).wait_send()
        part_copy(peer, t).wait_send()

    x_sends_done()

    def y_done(step, carry):
        a, b = spread(step)
        y_copy(a, b, g, t).wait_send()
        return carry

    lax.fori_loop(1, devices, y_done, 0)


def fused_layer(groups, lanes_tp, *args):
    args = list(args)
    for i in (8, 16, 17):
        args[i] = args[i].T
    for i in (18, 19):
        args[i] = args[i].swapaxes(1, 2)
    args = [a.reshape(1, -1) if a.ndim == 1 and a.dtype == F32 else a for a in args]
    spots = np.arange(HEADS * ROPE) % (ROPE // 2)
    args.append(jnp.asarray((rope_base ** (-2.0 * spots / ROPE))[None].astype(np.float32)))
    rows, width = args[0].shape
    own = args[14].shape[0]
    quarter = width // lanes_tp
    block = HEADS * VDIM // lanes_tp
    local = [
        pltpu.SMEM(a.shape, a.dtype) if i == 14 else pltpu.VMEM(a.shape, a.dtype)
        for i, a in enumerate(args)
    ]
    sem = pltpu.SemaphoreType.DMA
    return pl.pallas_call(
        functools.partial(layer_kernel, groups, lanes_tp),
        out_shape=jax.ShapeDtypeStruct((rows, quarter), F32),
        in_specs=[pl.BlockSpec(memory_space=pl.ANY)] * len(args),
        out_specs=pl.BlockSpec(memory_space=pltpu.VMEM),
        scratch_shapes=local
        + [
            sem((len(args),)),
            pltpu.VMEM((lanes_tp, 8, block), F32),
            pltpu.VMEM((lanes_tp, 8, block), F32),
            pltpu.VMEM((rows, block), F32),
            pltpu.VMEM((lanes_tp, rows, width), BF16),
            pltpu.VMEM((lanes_tp, rows, quarter), F32),
            pltpu.VMEM((groups, 2, rows, width // 2), BF16),
            pltpu.VMEM((groups, lanes_tp, rows, quarter), BF16),
            pltpu.VMEM((groups, lanes_tp, rows, quarter), BF16),
            sem((lanes_tp,)), sem((lanes_tp,)), sem((lanes_tp,)), sem((lanes_tp,)),
            sem((groups,)), sem((groups,)), sem((groups,)), sem((groups,)),
            sem((groups, lanes_tp)), sem((groups, lanes_tp)),
        ],
        compiler_params=pltpu.CompilerParams(
            collective_id=0, has_side_effects=True, vmem_limit_bytes=60 * 1024 * 1024
        ),
    )(*args).astype(BF16)


def pick_form(groups, lanes_tp, *args):
    rows = args[0].shape[0]
    if max(2, 4 * rows // (groups // 2)) < rows or lanes_tp % 2:
        return per_device(*args)
    return fused_layer(groups, lanes_tp, *args)


def solution(mesh):
    placed = (
        P("ep", None),
        P(),
        P(),
        P(),
        P(),
        P(),
        P(),
        P(),
        P(),
        P(),
        P(),
        P("tp", None),
        P(("ep", "tp"), None, None),
        P(("ep", "tp"), None, None),
        P(("ep", "tp")),
        P(),
        P("ep", None),
        P("ep", None),
        P("ep", None, "tp"),
        P("ep", None, "tp"),
        P("ep", "tp", None),
    )
    step = functools.partial(pick_form, mesh.shape["ep"], mesh.shape["tp"])
    return jax.shard_map(
        step, mesh=mesh, in_specs=placed, out_specs=P("ep", "tp"), check_vma=False
    )
```

```python
import functools

import jax
import jax.numpy as jnp
import numpy as np
from jax import lax
from jax.experimental import pallas as pl
from jax.experimental.pallas import tpu as pltpu
from jax.sharding import PartitionSpec as P

HEADS = 8
NOPE = 64
ROPE = 32
VDIM = 64
KVLORA = 128


eps = 1e-06
rope_base = 10000.0


def rms_scale(values, gain):
    return values * lax.rsqrt(jnp.mean(values * values, axis=-1, keepdims=True) + eps) * gain


def rotate(values, positions):
    width = values.shape[-1]
    middle = width // 2
    inverse = jnp.power(rope_base, -jnp.arange(0, width, 2).astype(jnp.float32) / width)
    angles = positions.astype(jnp.float32)[:, None] * inverse[None, :]
    angles = jnp.concatenate([angles, angles], axis=-1)
    target = (angles.shape[0],) + (1,) * (values.ndim - 2) + (width,)
    cosine = jnp.cos(angles).reshape(target)
    sine = jnp.sin(angles).reshape(target)
    turned = jnp.concatenate([-values[..., middle:], values[..., :middle]], axis=-1)
    return values * cosine + turned * sine


def route_slots(route_table, expert_count):
    flat_ids = route_table.reshape(-1)
    onehot = (flat_ids[:, None] == jnp.arange(expert_count, dtype=jnp.int32)[None, :]).astype(
        jnp.int32
    )
    before = jnp.cumsum(onehot, axis=0) - onehot
    return jnp.sum(before * onehot, axis=1).reshape(route_table.shape)


def unit_block(arrived, w_gate, w_up, w_down):
    gate_part = jnp.einsum("scd,df->scf", arrived, w_gate[0], preferred_element_type=jnp.float32)
    up_part = jnp.einsum("scd,df->scf", arrived, w_up[0], preferred_element_type=jnp.float32)
    inner = (jax.nn.silu(gate_part) * up_part).astype(jnp.bfloat16)
    block_term = jnp.einsum("scf,fd->scd", inner, w_down[0], preferred_element_type=jnp.float32)
    summed = lax.psum_scatter(
        block_term.astype(jnp.bfloat16), "tp", scatter_dimension=2, tiled=True
    )
    return lax.all_to_all(summed, "ep", split_axis=0, concat_axis=0, tiled=True)


def per_device(
    hidden_in,
    attn_gain,
    w_qdown,
    q_gain,
    w_qnope,
    w_qrope,
    w_kvdown,
    kv_gain,
    w_krope,
    w_ukey,
    w_uvalue,
    w_out,
    cache_latent,
    cache_rope,
    lengths,
    ffn_gain,
    routes,
    route_weights,
    w_gate,
    w_up,
    w_down,
):
    group_rows, width = hidden_in.shape
    own_count = lengths.shape[0]
    tp_rank = lax.axis_index("tp")
    score_scale = (NOPE + ROPE) ** (-0.5)
    own_rows = lax.dynamic_slice_in_dim(hidden_in, tp_rank * own_count, own_count, 0).astype(
        jnp.float32
    )
    normed = rms_scale(own_rows, attn_gain).astype(jnp.bfloat16)
    q_small = rms_scale(
        jnp.dot(normed, w_qdown, preferred_element_type=jnp.float32), q_gain
    ).astype(jnp.bfloat16)
    q_plain = (
        jnp.dot(q_small, w_qnope, preferred_element_type=jnp.float32)
        .astype(jnp.bfloat16)
        .reshape(own_count, HEADS, NOPE)
    )
    q_turned = rotate(
        jnp.dot(q_small, w_qrope, preferred_element_type=jnp.float32).reshape(
            own_count, HEADS, ROPE
        ),
        lengths,
    ).astype(jnp.bfloat16)
    q_latent = jnp.einsum(
        "shn,chn->shc",
        q_plain,
        w_ukey.reshape(KVLORA, HEADS, NOPE),
        preferred_element_type=jnp.float32,
    ).astype(jnp.bfloat16)
    new_latent = rms_scale(
        jnp.dot(normed, w_kvdown, preferred_element_type=jnp.float32), kv_gain
    ).astype(jnp.bfloat16)
    new_rope = rotate(jnp.dot(normed, w_krope, preferred_element_type=jnp.float32), lengths).astype(
        jnp.bfloat16
    )
    past_scores = (
        jnp.einsum("shc,spc->shp", q_latent, cache_latent, preferred_element_type=jnp.float32)
        + jnp.einsum("shr,srp->shp", q_turned, cache_rope, preferred_element_type=jnp.float32)
    ) * score_scale
    in_range = jnp.arange(cache_latent.shape[1])[None, None, :] < lengths[:, None, None]
    past_scores = jnp.where(in_range, past_scores, -1e30)
    fresh_score = (
        jnp.einsum("shc,sc->sh", q_latent, new_latent, preferred_element_type=jnp.float32)
        + jnp.einsum("shr,sr->sh", q_turned, new_rope, preferred_element_type=jnp.float32)
    ) * score_scale
    highest = jnp.maximum(jnp.max(past_scores, axis=-1), fresh_score)
    past_exp = jnp.exp(past_scores - highest[..., None])
    fresh_exp = jnp.exp(fresh_score - highest)
    divisor = jnp.sum(past_exp, axis=-1) + fresh_exp
    past_prob = (past_exp / divisor[..., None]).astype(jnp.bfloat16)
    fresh_prob = (fresh_exp / divisor).astype(jnp.bfloat16)
    latent_mix = (
        jnp.einsum("shp,spc->shc", past_prob, cache_latent, preferred_element_type=jnp.float32)
        + fresh_prob.astype(jnp.float32)[..., None] * new_latent.astype(jnp.float32)[:, None, :]
    ).astype(jnp.bfloat16)
    head_values = (
        jnp.einsum(
            "shc,chv->shv",
            latent_mix,
            w_uvalue.reshape(KVLORA, HEADS, VDIM),
            preferred_element_type=jnp.float32,
        )
        .astype(jnp.bfloat16)
        .reshape(own_count, HEADS * VDIM)
    )
    by_heads = lax.all_to_all(head_values, "tp", split_axis=1, concat_axis=0, tiled=True)
    attended = lax.psum(
        jnp.dot(by_heads, w_out, preferred_element_type=jnp.float32).astype(jnp.bfloat16), "tp"
    ).astype(jnp.float32)
    residual = hidden_in.astype(jnp.float32) + attended
    normed_two = rms_scale(residual, ffn_gain).astype(jnp.bfloat16)
    unit_count = lax.axis_size("ep")
    expert_count = unit_count // 2
    capacity = max(2, 4 * group_rows // expert_count)
    quarter = width // lax.axis_size("tp")
    slots = route_slots(routes, expert_count)
    expert_of_unit = jnp.arange(unit_count, dtype=jnp.int32) // 2
    slot_range = jnp.arange(capacity, dtype=jnp.int32)
    chosen = (routes[None, None, :, :] == expert_of_unit[:, None, None, None]) & (
        slots[None, None, :, :] == slot_range[None, :, None, None]
    )
    chooser = jnp.sum(chosen.astype(jnp.int32), axis=-1).astype(jnp.bfloat16)
    outgoing = jnp.einsum(
        "ucr,rd->ucd", chooser, normed_two, preferred_element_type=jnp.float32
    ).astype(jnp.bfloat16)
    returned = unit_block(
        lax.all_to_all(outgoing, "ep", split_axis=0, concat_axis=0, tiled=True),
        w_gate,
        w_up,
        w_down,
    )
    stacked = returned.reshape(unit_count * capacity, quarter)
    first_row = routes * (2 * capacity) + slots
    first_half = stacked[first_row].astype(jnp.float32)
    second_half = stacked[first_row + capacity].astype(jnp.float32)
    blended = jnp.sum(route_weights[..., None] * (first_half + second_half), axis=1)
    own_columns = lax.dynamic_slice_in_dim(residual, tp_rank * quarter, quarter, 1)
    return (own_columns + blended).astype(jnp.bfloat16)


LINK = pl.DeviceIdType.MESH
F32 = jnp.float32
BF16 = jnp.bfloat16


def mm(a, b):
    return jnp.dot(a, b, preferred_element_type=F32)


def mm_nt(a, b):
    return lax.dot_general(a, b, (((1,), (1,)), ((), ())), preferred_element_type=F32)


def iota(shape, dim):
    return lax.broadcasted_iota(jnp.int32, shape, dim)


def layer_kernel(groups, lanes_tp, *refs):
    names = 22
    hbm, out_ref = refs[:names], refs[names]
    local = refs[names + 1 : 2 * names + 1]
    (
        load_sem, hv_send, hv_recv, rows_buf, part, res_buf, x_buf, y_send, y_recv,
        hv_ss, hv_rs, part_ss, part_rs, x_ss, x_rs, f_ss, f_rs, y_ss, y_rs,
    ) = refs[2 * names + 1 :]
    (
        hidden, attn_gain, w_qdown, q_gain, w_qnope, w_qrope, w_kvdown, kv_gain, w_krope,
        w_ukey, w_uvalue, w_out, cache_latent, cache_rope, lengths, ffn_gain, routes,
        route_weights, w_gate, w_up, w_down, inverse,
    ) = local
    g, t = lax.axis_index("ep"), lax.axis_index("tp")
    devices = groups * lanes_tp
    me = g * lanes_tp + t

    barrier = pltpu.get_barrier_semaphore()

    def ring(step):
        return lax.rem(g + step, groups)

    peers = [lax.rem(t + i, lanes_tp) for i in range(1, lanes_tp)]
    for peer in peers:
        pl.semaphore_signal(barrier, inc=1, device_id=(g, peer), device_id_type=LINK)
    for i in range(1, groups):
        pl.semaphore_signal(barrier, inc=1, device_id=(ring(i), t), device_id_type=LINK)

    loads = [
        pltpu.make_async_copy(hbm[i], local[i], load_sem.at[i]) for i in range(names)
    ]
    order = [0, 1, 2, 3, 14, 21, 6, 8, 7, 4, 5, 9, 12, 13, 10, 11, 15, 16, 17, 18, 19, 20]
    for i in order:
        loads[i].start()

    own = lengths.shape[0]
    rows, width = hidden.shape
    quarter = width // lanes_tp
    pad = 8

    for i in (0, 1, 2, 3):
        loads[i].wait()
    pick = (iota((pad, rows), 1) == iota((pad, rows), 0) + t * own) & (
        iota((pad, rows), 0) < own
    )
    mine = mm(jnp.where(pick, 1.0, 0.0).astype(BF16), hidden[...])
    normed = rms_scale(mine, attn_gain[...]).astype(BF16)
    q_small = rms_scale(mm(normed, w_qdown[...]), q_gain[...]).astype(BF16)
    for i in (14, 21, 6, 8, 7, 4, 5):
        loads[i].wait()
    position = jnp.zeros((pad, 1), jnp.int32)
    for s in range(own):
        position = jnp.where(iota((pad, 1), 0) == s, lengths[s], position)
    angles = position.astype(F32) * inverse[...]
    cosine, sine = jnp.cos(angles), jnp.sin(angles)
    new_latent = rms_scale(mm(normed, w_kvdown[...]), kv_gain[...]).astype(BF16).astype(F32)
    rope_key = mm_nt(normed, w_krope[...])
    turned_key = jnp.concatenate([-rope_key[:, ROPE // 2 :], rope_key[:, : ROPE // 2]], axis=1)
    new_rope = rope_key * cosine[:, :ROPE] + turned_key * sine[:, :ROPE]
    new_rope = new_rope.astype(BF16).astype(F32)
    q_plain = mm(q_small, w_qnope[...]).astype(BF16).astype(F32)
    q_rope = mm(q_small, w_qrope[...])
    span = HEADS * ROPE
    first = (iota((pad, span), 1) & (ROPE - 1)) < ROPE // 2
    turned = jnp.where(
        first, -pltpu.roll(q_rope, span - ROPE // 2, 1), pltpu.roll(q_rope, ROPE // 2, 1)
    )
    q_turned = (q_rope * cosine + turned * sine).astype(BF16).astype(F32)
    plain_mask = iota((HEADS, HEADS * NOPE), 1) // NOPE == iota((HEADS, HEADS * NOPE), 0)
    rope_mask = iota((HEADS, span), 1) // ROPE == iota((HEADS, span), 0)
    plain_rows = jnp.concatenate(
        [jnp.where(plain_mask, q_plain[s : s + 1, :], 0.0) for s in range(own)], axis=0
    ).astype(BF16)
    rope_rows = jnp.concatenate(
        [jnp.where(rope_mask, q_turned[s : s + 1, :], 0.0) for s in range(own)], axis=0
    ).astype(BF16)
    fold = ((iota((span, ROPE), 0) & (ROPE - 1)) == iota((span, ROPE), 1)).astype(F32)
    q_heads = mm(rope_rows, fold.astype(BF16))
    loads[9].wait()
    q_latent = mm_nt(plain_rows, w_ukey[...]).astype(BF16)
    loads[12].wait()
    loads[13].wait()
    scale = (NOPE + ROPE) ** (-0.5)
    cache = cache_latent.shape[1]
    mixes = []
    for s in range(own):
        heads = slice(s * HEADS, (s + 1) * HEADS)
        ql, qr = q_latent[heads], q_heads[heads]
        scores = (mm_nt(ql, cache_latent[s]) + mm(qr.astype(BF16), cache_rope[s])) * scale
        scores = jnp.where(iota((HEADS, cache), 1) < lengths[s], scores, -1e30)
        fresh = (
            jnp.sum(ql.astype(F32) * new_latent[s : s + 1, :], axis=1, keepdims=True)
            + jnp.sum(qr * new_rope[s : s + 1, :], axis=1, keepdims=True)
        ) * scale
        highest = jnp.maximum(jnp.max(scores, axis=1, keepdims=True), fresh)
        past_exp = jnp.exp(scores - highest)
        fresh_exp = jnp.exp(fresh - highest)
        divisor = jnp.sum(past_exp, axis=1, keepdims=True) + fresh_exp
        past_prob = (past_exp / divisor).astype(BF16)
        fresh_prob = (fresh_exp / divisor).astype(BF16).astype(F32)
        mixes.append(mm(past_prob, cache_latent[s]) + fresh_prob * new_latent[s : s + 1, :])
    loads[10].wait()
    mix = jnp.concatenate(mixes, axis=0).astype(BF16)
    values = mm(mix, w_uvalue[...])
    value_mask = iota((HEADS, HEADS * VDIM), 1) // VDIM == iota((HEADS, HEADS * VDIM), 0)
    block = HEADS * VDIM // lanes_tp
    for s in range(own):
        row = jnp.sum(
            jnp.where(value_mask, values[s * HEADS : (s + 1) * HEADS], 0.0), axis=0, keepdims=True
        )
        row = row.astype(BF16).astype(F32)
        for i in range(lanes_tp):
            hv_send[i, s : s + 1, :] = row[:, i * block : (i + 1) * block]

    pl.semaphore_wait(barrier, groups + lanes_tp - 2)

    def hv_copy(peer, slot):
        return pltpu.make_async_remote_copy(
            hv_send.at[peer], hv_recv.at[slot], hv_ss.at[peer], hv_rs.at[slot],
            device_id=(g, peer), device_id_type=LINK,
        )

    for peer in peers:
        hv_copy(peer, t).start()
    hv_recv[t] = hv_send[t]
    loads[11].wait()
    loads[15].wait()
    for peer in peers:
        hv_copy(peer, peer).wait_recv()
    for i in range(lanes_tp):
        rows_buf[i * own : (i + 1) * own, :] = hv_recv[i, :own, :]
    part[t] = mm(rows_buf[...].astype(BF16), w_out[...]).astype(BF16)

    def part_copy(peer, slot):
        return pltpu.make_async_remote_copy(
            part.at[slot], part.at[slot], part_ss.at[peer], part_rs.at[slot],
            device_id=(g, peer), device_id_type=LINK,
        )

    for peer in peers:
        part_copy(peer, t).start()
    for peer in peers:
        part_copy(peer, peer).wait_recv()
    attended = part[0].astype(F32)
    for i in range(1, lanes_tp):
        attended = attended + part[i].astype(F32)
    residual = hidden[...].astype(F32) + attended
    normed_two = rms_scale(residual, ffn_gain[...]).astype(BF16)
    for i in range(lanes_tp):
        res_buf[i] = residual[:, i * quarter : (i + 1) * quarter]

    half_width = width // 2
    for i in range(2):
        x_buf[g, i] = normed_two[:, i * half_width : (i + 1) * half_width]

    mine_half = lax.rem(t, 2)
    partner = t + 1 - 2 * mine_half

    def x_copy(other, slot):
        return pltpu.make_async_remote_copy(
            x_buf.at[slot, mine_half], x_buf.at[slot, mine_half], x_ss.at[other], x_rs.at[slot],
            device_id=(other, t), device_id_type=LINK,
        )

    def f_copy(slot, half):
        return pltpu.make_async_remote_copy(
            x_buf.at[slot, half], x_buf.at[slot, half], f_ss.at[slot], f_rs.at[slot],
            device_id=(g, partner), device_id_type=LINK,
        )

    near = sorted(range(1, groups), key=lambda i: min(i, groups - i))
    for i in near:
        x_copy(ring(i), g).start()
    for i in (16, 17, 18, 19, 20):
        loads[i].wait()
    for i in near:
        x_copy(ring(groups - i), ring(groups - i)).wait_recv()
        f_copy(ring(groups - i), mine_half).start()
    for i in near:
        f_copy(ring(i), 1 - mine_half).wait_recv()

    def x_sends_done():
        for i in near:
            x_copy(ring(i), g).wait_send()
            f_copy(ring(i), mine_half).wait_send()

    tokens = groups * rows
    gate = jnp.zeros((tokens, w_gate.shape[1]), F32)
    up = jnp.zeros((tokens, w_gate.shape[1]), F32)
    for i in range(2):
        piece = x_buf[:, i].reshape(tokens, half_width)
        depth = slice(i * half_width, (i + 1) * half_width)
        gate = gate + mm_nt(piece, w_gate[0, :, depth])
        up = up + mm_nt(piece, w_up[0, :, depth])
    inner = (gate / (1.0 + jnp.exp(-gate)) * up).astype(BF16)
    for i in range(lanes_tp):
        term = mm(inner, w_down[0, :, i * quarter : (i + 1) * quarter]).astype(BF16)
        y_send[:, i] = term.reshape(groups, rows, quarter)

    same = iota((rows, rows), 0) == iota((rows, rows), 1)
    weights = []
    for e in range(groups // 2):
        flat = jnp.sum(
            jnp.where(routes[...] == e, route_weights[...], 0.0), axis=0, keepdims=True
        )
        weights.append(jnp.sum(jnp.where(same, flat, 0.0), axis=1, keepdims=True))

    def y_copy(other_g, other_t, slot_g, slot_t):
        return pltpu.make_async_remote_copy(
            y_send.at[other_g, other_t], y_recv.at[slot_g, slot_t],
            y_ss.at[other_g, other_t], y_rs.at[slot_g, slot_t],
            device_id=(other_g, other_t), device_id_type=LINK,
        )

    def spread(step):
        peer = lax.rem(me + step, devices)
        return peer // lanes_tp, lax.rem(peer, lanes_tp)

    def y_start(step, carry):
        a, b = spread(step)
        y_copy(a, b, g, t).start()
        return carry

    lax.fori_loop(1, devices, y_start, 0)
    y_recv[g, t] = y_send[g, t]

    def y_wait(step, carry):
        a, b = spread(step)
        y_copy(a, b, a, b).wait_recv()
        return carry

    lax.fori_loop(1, devices, y_wait, 0)
    total = res_buf[t]
    for u in range(groups):
        half = y_recv[u, 0].astype(F32)
        for i in range(1, lanes_tp):
            half = half + y_recv[u, i].astype(F32)
        total = total + weights[u // 2] * half.astype(BF16).astype(F32)
    out_ref[...] = total

    for peer in peers:
        hv_copy(peer, t).wait_send()
        part_copy(peer, t).wait_send()

    x_sends_done()

    def y_done(step, carry):
        a, b = spread(step)
        y_copy(a, b, g, t).wait_send()
        return carry

    lax.fori_loop(1, devices, y_done, 0)


def fused_layer(groups, lanes_tp, *args):
    args = list(args)
    for i in (8, 16, 17):
        args[i] = args[i].T
    for i in (18, 19):
        args[i] = args[i].swapaxes(1, 2)
    args = [a.reshape(1, -1) if a.ndim == 1 and a.dtype == F32 else a for a in args]
    spots = np.arange(HEADS * ROPE) % (ROPE // 2)
    args.append(jnp.asarray((rope_base ** (-2.0 * spots / ROPE))[None].astype(np.float32)))
    rows, width = args[0].shape
    own = args[14].shape[0]
    quarter = width // lanes_tp
    block = HEADS * VDIM // lanes_tp
    local = [
        pltpu.SMEM(a.shape, a.dtype) if i == 14 else pltpu.VMEM(a.shape, a.dtype)
        for i, a in enumerate(args)
    ]
    sem = pltpu.SemaphoreType.DMA
    return pl.pallas_call(
        functools.partial(layer_kernel, groups, lanes_tp),
        out_shape=pltpu.VMEM((rows, quarter), F32),
        in_specs=[pl.BlockSpec(memory_space=pl.ANY)] * len(args),
        out_specs=pl.BlockSpec(memory_space=pltpu.VMEM),
        scratch_shapes=local
        + [
            sem((len(args),)),
            pltpu.VMEM((lanes_tp, 8, block), F32),
            pltpu.VMEM((lanes_tp, 8, block), F32),
            pltpu.VMEM((rows, block), F32),
            pltpu.VMEM((lanes_tp, rows, width), BF16),
            pltpu.VMEM((lanes_tp, rows, quarter), F32),
            pltpu.VMEM((groups, 2, rows, width // 2), BF16),
            pltpu.VMEM((groups, lanes_tp, rows, quarter), BF16),
            pltpu.VMEM((groups, lanes_tp, rows, quarter), BF16),
            sem((lanes_tp,)), sem((lanes_tp,)), sem((lanes_tp,)), sem((lanes_tp,)),
            sem((groups,)), sem((groups,)), sem((groups,)), sem((groups,)),
            sem((groups, lanes_tp)), sem((groups, lanes_tp)),
        ],
        compiler_params=pltpu.CompilerParams(
            collective_id=0, has_side_effects=True, vmem_limit_bytes=60 * 1024 * 1024
        ),
    )(*args).astype(BF16)


def pick_form(groups, lanes_tp, *args):
    rows = args[0].shape[0]
    if max(2, 4 * rows // (groups // 2)) < rows or lanes_tp % 2:
        return per_device(*args)
    return fused_layer(groups, lanes_tp, *args)


def solution(mesh):
    placed = (
        P("ep", None),
        P(),
        P(),
        P(),
        P(),
        P(),
        P(),
        P(),
        P(),
        P(),
        P(),
        P("tp", None),
        P(("ep", "tp"), None, None),
        P(("ep", "tp"), None, None),
        P(("ep", "tp")),
        P(),
        P("ep", None),
        P("ep", None),
        P("ep", None, "tp"),
        P("ep", None, "tp"),
        P("ep", "tp", None),
    )
    step = functools.partial(pick_form, mesh.shape["ep"], mesh.shape["tp"])
    return jax.shard_map(
        step, mesh=mesh, in_specs=placed, out_specs=P("ep", "tp"), check_vma=False
    )
```

```python
import functools

import jax
import jax.numpy as jnp
import numpy as np
from jax import lax
from jax.experimental import pallas as pl
from jax.experimental.pallas import tpu as pltpu
from jax.sharding import PartitionSpec as P

HEADS = 8
NOPE = 64
ROPE = 32
VDIM = 64
KVLORA = 128


eps = 1e-06
rope_base = 10000.0


def rms_scale(values, gain):
    return values * lax.rsqrt(jnp.mean(values * values, axis=-1, keepdims=True) + eps) * gain


def rotate(values, positions):
    width = values.shape[-1]
    middle = width // 2
    inverse = jnp.power(rope_base, -jnp.arange(0, width, 2).astype(jnp.float32) / width)
    angles = positions.astype(jnp.float32)[:, None] * inverse[None, :]
    angles = jnp.concatenate([angles, angles], axis=-1)
    target = (angles.shape[0],) + (1,) * (values.ndim - 2) + (width,)
    cosine = jnp.cos(angles).reshape(target)
    sine = jnp.sin(angles).reshape(target)
    turned = jnp.concatenate([-values[..., middle:], values[..., :middle]], axis=-1)
    return values * cosine + turned * sine


def route_slots(route_table, expert_count):
    flat_ids = route_table.reshape(-1)
    onehot = (flat_ids[:, None] == jnp.arange(expert_count, dtype=jnp.int32)[None, :]).astype(
        jnp.int32
    )
    before = jnp.cumsum(onehot, axis=0) - onehot
    return jnp.sum(before * onehot, axis=1).reshape(route_table.shape)


def unit_block(arrived, w_gate, w_up, w_down):
    gate_part = jnp.einsum("scd,df->scf", arrived, w_gate[0], preferred_element_type=jnp.float32)
    up_part = jnp.einsum("scd,df->scf", arrived, w_up[0], preferred_element_type=jnp.float32)
    inner = (jax.nn.silu(gate_part) * up_part).astype(jnp.bfloat16)
    block_term = jnp.einsum("scf,fd->scd", inner, w_down[0], preferred_element_type=jnp.float32)
    summed = lax.psum_scatter(
        block_term.astype(jnp.bfloat16), "tp", scatter_dimension=2, tiled=True
    )
    return lax.all_to_all(summed, "ep", split_axis=0, concat_axis=0, tiled=True)


def per_device(
    hidden_in,
    attn_gain,
    w_qdown,
    q_gain,
    w_qnope,
    w_qrope,
    w_kvdown,
    kv_gain,
    w_krope,
    w_ukey,
    w_uvalue,
    w_out,
    cache_latent,
    cache_rope,
    lengths,
    ffn_gain,
    routes,
    route_weights,
    w_gate,
    w_up,
    w_down,
):
    group_rows, width = hidden_in.shape
    own_count = lengths.shape[0]
    tp_rank = lax.axis_index("tp")
    score_scale = (NOPE + ROPE) ** (-0.5)
    own_rows = lax.dynamic_slice_in_dim(hidden_in, tp_rank * own_count, own_count, 0).astype(
        jnp.float32
    )
    normed = rms_scale(own_rows, attn_gain).astype(jnp.bfloat16)
    q_small = rms_scale(
        jnp.dot(normed, w_qdown, preferred_element_type=jnp.float32), q_gain
    ).astype(jnp.bfloat16)
    q_plain = (
        jnp.dot(q_small, w_qnope, preferred_element_type=jnp.float32)
        .astype(jnp.bfloat16)
        .reshape(own_count, HEADS, NOPE)
    )
    q_turned = rotate(
        jnp.dot(q_small, w_qrope, preferred_element_type=jnp.float32).reshape(
            own_count, HEADS, ROPE
        ),
        lengths,
    ).astype(jnp.bfloat16)
    q_latent = jnp.einsum(
        "shn,chn->shc",
        q_plain,
        w_ukey.reshape(KVLORA, HEADS, NOPE),
        preferred_element_type=jnp.float32,
    ).astype(jnp.bfloat16)
    new_latent = rms_scale(
        jnp.dot(normed, w_kvdown, preferred_element_type=jnp.float32), kv_gain
    ).astype(jnp.bfloat16)
    new_rope = rotate(jnp.dot(normed, w_krope, preferred_element_type=jnp.float32), lengths).astype(
        jnp.bfloat16
    )
    past_scores = (
        jnp.einsum("shc,spc->shp", q_latent, cache_latent, preferred_element_type=jnp.float32)
        + jnp.einsum("shr,srp->shp", q_turned, cache_rope, preferred_element_type=jnp.float32)
    ) * score_scale
    in_range = jnp.arange(cache_latent.shape[1])[None, None, :] < lengths[:, None, None]
    past_scores = jnp.where(in_range, past_scores, -1e30)
    fresh_score = (
        jnp.einsum("shc,sc->sh", q_latent, new_latent, preferred_element_type=jnp.float32)
        + jnp.einsum("shr,sr->sh", q_turned, new_rope, preferred_element_type=jnp.float32)
    ) * score_scale
    highest = jnp.maximum(jnp.max(past_scores, axis=-1), fresh_score)
    past_exp = jnp.exp(past_scores - highest[..., None])
    fresh_exp = jnp.exp(fresh_score - highest)
    divisor = jnp.sum(past_exp, axis=-1) + fresh_exp
    past_prob = (past_exp / divisor[..., None]).astype(jnp.bfloat16)
    fresh_prob = (fresh_exp / divisor).astype(jnp.bfloat16)
    latent_mix = (
        jnp.einsum("shp,spc->shc", past_prob, cache_latent, preferred_element_type=jnp.float32)
        + fresh_prob.astype(jnp.float32)[..., None] * new_latent.astype(jnp.float32)[:, None, :]
    ).astype(jnp.bfloat16)
    head_values = (
        jnp.einsum(
            "shc,chv->shv",
            latent_mix,
            w_uvalue.reshape(KVLORA, HEADS, VDIM),
            preferred_element_type=jnp.float32,
        )
        .astype(jnp.bfloat16)
        .reshape(own_count, HEADS * VDIM)
    )
    by_heads = lax.all_to_all(head_values, "tp", split_axis=1, concat_axis=0, tiled=True)
    attended = lax.psum(
        jnp.dot(by_heads, w_out, preferred_element_type=jnp.float32).astype(jnp.bfloat16), "tp"
    ).astype(jnp.float32)
    residual = hidden_in.astype(jnp.float32) + attended
    normed_two = rms_scale(residual, ffn_gain).astype(jnp.bfloat16)
    unit_count = lax.axis_size("ep")
    expert_count = unit_count // 2
    capacity = max(2, 4 * group_rows // expert_count)
    quarter = width // lax.axis_size("tp")
    slots = route_slots(routes, expert_count)
    expert_of_unit = jnp.arange(unit_count, dtype=jnp.int32) // 2
    slot_range = jnp.arange(capacity, dtype=jnp.int32)
    chosen = (routes[None, None, :, :] == expert_of_unit[:, None, None, None]) & (
        slots[None, None, :, :] == slot_range[None, :, None, None]
    )
    chooser = jnp.sum(chosen.astype(jnp.int32), axis=-1).astype(jnp.bfloat16)
    outgoing = jnp.einsum(
        "ucr,rd->ucd", chooser, normed_two, preferred_element_type=jnp.float32
    ).astype(jnp.bfloat16)
    returned = unit_block(
        lax.all_to_all(outgoing, "ep", split_axis=0, concat_axis=0, tiled=True),
        w_gate,
        w_up,
        w_down,
    )
    stacked = returned.reshape(unit_count * capacity, quarter)
    first_row = routes * (2 * capacity) + slots
    first_half = stacked[first_row].astype(jnp.float32)
    second_half = stacked[first_row + capacity].astype(jnp.float32)
    blended = jnp.sum(route_weights[..., None] * (first_half + second_half), axis=1)
    own_columns = lax.dynamic_slice_in_dim(residual, tp_rank * quarter, quarter, 1)
    return (own_columns + blended).astype(jnp.bfloat16)


LINK = pl.DeviceIdType.MESH
F32 = jnp.float32
BF16 = jnp.bfloat16


def mm(a, b):
    return jnp.dot(a, b, preferred_element_type=F32)


def mm_nt(a, b):
    return lax.dot_general(a, b, (((1,), (1,)), ((), ())), preferred_element_type=F32)


def iota(shape, dim):
    return lax.broadcasted_iota(jnp.int32, shape, dim)


def layer_kernel(groups, lanes_tp, *refs):
    names = 22
    hbm, out_ref = refs[:names], refs[names]
    local = refs[names + 1 : 2 * names + 1]
    (
        load_sem, hv_send, hv_recv, rows_buf, part, res_buf, x_buf, y_send, p_recv, z_buf, y_recv,
        hv_ss, hv_rs, part_ss, part_rs, x_ss, x_rs, f_ss, f_rs, p_ss, p_rs, y_ss, y_rs,
    ) = refs[2 * names + 1 :]
    (
        hidden, attn_gain, w_qdown, q_gain, w_qnope, w_qrope, w_kvdown, kv_gain, w_krope,
        w_ukey, w_uvalue, w_out, cache_latent, cache_rope, lengths, ffn_gain, routes,
        route_weights, w_gate, w_up, w_down, inverse,
    ) = local
    g, t = lax.axis_index("ep"), lax.axis_index("tp")

    barrier = pltpu.get_barrier_semaphore()

    def ring(step):
        return lax.rem(g + step, groups)

    peers = [lax.rem(t + i, lanes_tp) for i in range(1, lanes_tp)]
    for peer in peers:
        pl.semaphore_signal(barrier, inc=1, device_id=(g, peer), device_id_type=LINK)
    for i in range(1, groups):
        pl.semaphore_signal(barrier, inc=1, device_id=(ring(i), t), device_id_type=LINK)

    loads = [
        pltpu.make_async_copy(hbm[i], local[i], load_sem.at[i]) for i in range(names)
    ]
    order = [0, 1, 2, 3, 14, 21, 6, 8, 7, 4, 5, 9, 12, 13, 10, 11, 15, 16, 17, 18, 19, 20]
    for i in order:
        loads[i].start()

    own = lengths.shape[0]
    rows, width = hidden.shape
    quarter = width // lanes_tp
    pad = 8

    for i in (0, 1, 2, 3):
        loads[i].wait()
    pick = (iota((pad, rows), 1) == iota((pad, rows), 0) + t * own) & (
        iota((pad, rows), 0) < own
    )
    mine = mm(jnp.where(pick, 1.0, 0.0).astype(BF16), hidden[...])
    normed = rms_scale(mine, attn_gain[...]).astype(BF16)
    q_small = rms_scale(mm(normed, w_qdown[...]), q_gain[...]).astype(BF16)
    for i in (14, 21, 6, 8, 7, 4, 5):
        loads[i].wait()
    position = jnp.zeros((pad, 1), jnp.int32)
    for s in range(own):
        position = jnp.where(iota((pad, 1), 0) == s, lengths[s], position)
    angles = position.astype(F32) * inverse[...]
    cosine, sine = jnp.cos(angles), jnp.sin(angles)
    new_latent = rms_scale(mm(normed, w_kvdown[...]), kv_gain[...]).astype(BF16).astype(F32)
    rope_key = mm_nt(normed, w_krope[...])
    turned_key = jnp.concatenate([-rope_key[:, ROPE // 2 :], rope_key[:, : ROPE // 2]], axis=1)
    new_rope = rope_key * cosine[:, :ROPE] + turned_key * sine[:, :ROPE]
    new_rope = new_rope.astype(BF16).astype(F32)
    q_plain = mm(q_small, w_qnope[...]).astype(BF16).astype(F32)
    q_rope = mm(q_small, w_qrope[...])
    span = HEADS * ROPE
    first = (iota((pad, span), 1) & (ROPE - 1)) < ROPE // 2
    turned = jnp.where(
        first, -pltpu.roll(q_rope, span - ROPE // 2, 1), pltpu.roll(q_rope, ROPE // 2, 1)
    )
    q_turned = (q_rope * cosine + turned * sine).astype(BF16).astype(F32)
    plain_mask = iota((HEADS, HEADS * NOPE), 1) // NOPE == iota((HEADS, HEADS * NOPE), 0)
    rope_mask = iota((HEADS, span), 1) // ROPE == iota((HEADS, span), 0)
    plain_rows = jnp.concatenate(
        [jnp.where(plain_mask, q_plain[s : s + 1, :], 0.0) for s in range(own)], axis=0
    ).astype(BF16)
    rope_rows = jnp.concatenate(
        [jnp.where(rope_mask, q_turned[s : s + 1, :], 0.0) for s in range(own)], axis=0
    ).astype(BF16)
    fold = ((iota((span, ROPE), 0) & (ROPE - 1)) == iota((span, ROPE), 1)).astype(F32)
    q_heads = mm(rope_rows, fold.astype(BF16))
    loads[9].wait()
    q_latent = mm_nt(plain_rows, w_ukey[...]).astype(BF16)
    loads[12].wait()
    loads[13].wait()
    scale = (NOPE + ROPE) ** (-0.5)
    cache = cache_latent.shape[1]
    mixes = []
    for s in range(own):
        heads = slice(s * HEADS, (s + 1) * HEADS)
        ql, qr = q_latent[heads], q_heads[heads]
        scores = (mm_nt(ql, cache_latent[s]) + mm(qr.astype(BF16), cache_rope[s])) * scale
        scores = jnp.where(iota((HEADS, cache), 1) < lengths[s], scores, -1e30)
        fresh = (
            jnp.sum(ql.astype(F32) * new_latent[s : s + 1, :], axis=1, keepdims=True)
            + jnp.sum(qr * new_rope[s : s + 1, :], axis=1, keepdims=True)
        ) * scale
        highest = jnp.maximum(jnp.max(scores, axis=1, keepdims=True), fresh)
        past_exp = jnp.exp(scores - highest)
        fresh_exp = jnp.exp(fresh - highest)
        divisor = jnp.sum(past_exp, axis=1, keepdims=True) + fresh_exp
        past_prob = (past_exp / divisor).astype(BF16)
        fresh_prob = (fresh_exp / divisor).astype(BF16).astype(F32)
        mixes.append(mm(past_prob, cache_latent[s]) + fresh_prob * new_latent[s : s + 1, :])
    loads[10].wait()
    mix = jnp.concatenate(mixes, axis=0).astype(BF16)
    values = mm(mix, w_uvalue[...])
    value_mask = iota((HEADS, HEADS * VDIM), 1) // VDIM == iota((HEADS, HEADS * VDIM), 0)
    block = HEADS * VDIM // lanes_tp
    for s in range(own):
        row = jnp.sum(
            jnp.where(value_mask, values[s * HEADS : (s + 1) * HEADS], 0.0), axis=0, keepdims=True
        )
        row = row.astype(BF16).astype(F32)
        for i in range(lanes_tp):
            hv_send[i, s : s + 1, :] = row[:, i * block : (i + 1) * block]

    pl.semaphore_wait(barrier, groups + lanes_tp - 2)

    def hv_copy(peer, slot):
        return pltpu.make_async_remote_copy(
            hv_send.at[peer], hv_recv.at[slot], hv_ss.at[peer], hv_rs.at[slot],
            device_id=(g, peer), device_id_type=LINK,
        )

    for peer in peers:
        hv_copy(peer, t).start()
    hv_recv[t] = hv_send[t]
    loads[11].wait()
    loads[15].wait()
    for peer in peers:
        hv_copy(peer, peer).wait_recv()
    for i in range(lanes_tp):
        rows_buf[i * own : (i + 1) * own, :] = hv_recv[i, :own, :]
    part[t] = mm(rows_buf[...].astype(BF16), w_out[...]).astype(BF16)

    def part_copy(peer, slot):
        return pltpu.make_async_remote_copy(
            part.at[slot], part.at[slot], part_ss.at[peer], part_rs.at[slot],
            device_id=(g, peer), device_id_type=LINK,
        )

    for peer in peers:
        part_copy(peer, t).start()
    for peer in peers:
        part_copy(peer, peer).wait_recv()
    attended = part[0].astype(F32)
    for i in range(1, lanes_tp):
        attended = attended + part[i].astype(F32)
    residual = hidden[...].astype(F32) + attended
    normed_two = rms_scale(residual, ffn_gain[...]).astype(BF16)
    for i in range(lanes_tp):
        res_buf[i] = residual[:, i * quarter : (i + 1) * quarter]

    half_width = width // 2
    for i in range(2):
        x_buf[g, i] = normed_two[:, i * half_width : (i + 1) * half_width]

    mine_half = lax.rem(t, 2)
    partner = t + 1 - 2 * mine_half

    def x_copy(other, slot):
        return pltpu.make_async_remote_copy(
            x_buf.at[slot, mine_half], x_buf.at[slot, mine_half], x_ss.at[other], x_rs.at[slot],
            device_id=(other, t), device_id_type=LINK,
        )

    def f_copy(slot, half):
        return pltpu.make_async_remote_copy(
            x_buf.at[slot, half], x_buf.at[slot, half], f_ss.at[slot], f_rs.at[slot],
            device_id=(g, partner), device_id_type=LINK,
        )

    near = sorted(range(1, groups), key=lambda i: min(i, groups - i))
    for i in near:
        x_copy(ring(i), g).start()
    for i in (16, 17, 18, 19, 20):
        loads[i].wait()
    for i in near:
        x_copy(ring(groups - i), ring(groups - i)).wait_recv()
        f_copy(ring(groups - i), mine_half).start()
    for i in near:
        f_copy(ring(i), 1 - mine_half).wait_recv()

    def x_sends_done():
        for i in near:
            x_copy(ring(i), g).wait_send()
            f_copy(ring(i), mine_half).wait_send()

    tokens = groups * rows
    gate = jnp.zeros((tokens, w_gate.shape[1]), F32)
    up = jnp.zeros((tokens, w_gate.shape[1]), F32)
    for i in range(2):
        piece = x_buf[:, i].reshape(tokens, half_width)
        depth = slice(i * half_width, (i + 1) * half_width)
        gate = gate + mm_nt(piece, w_gate[0, :, depth])
        up = up + mm_nt(piece, w_up[0, :, depth])
    inner = (gate / (1.0 + jnp.exp(-gate)) * up).astype(BF16)
    pairs = lanes_tp // 2

    def p_copy(j):
        return pltpu.make_async_remote_copy(
            y_send.at[0, j], p_recv.at[j], p_ss.at[j], p_rs.at[j],
            device_id=(g, partner), device_id_type=LINK,
        )

    for k, parity in enumerate((1 - mine_half, mine_half)):
        for j in range(pairs):
            start = pl.multiple_of((2 * j + parity) * quarter, quarter)
            term = mm(inner, w_down[0, :, pl.ds(start, quarter)]).astype(BF16)
            y_send[k, j] = term.reshape(groups, rows, quarter)
            if k == 0:
                p_copy(j).start()

    same = iota((rows, rows), 0) == iota((rows, rows), 1)
    weights = []
    for e in range(groups // 2):
        flat = jnp.sum(
            jnp.where(routes[...] == e, route_weights[...], 0.0), axis=0, keepdims=True
        )
        weights.append(jnp.sum(jnp.where(same, flat, 0.0), axis=1, keepdims=True))

    chip = t // 2

    def y_copy(other, j, slot_g, slot_j):
        return pltpu.make_async_remote_copy(
            z_buf.at[j, other], y_recv.at[slot_g, slot_j],
            y_ss.at[other, j], y_rs.at[slot_g, slot_j],
            device_id=(other, 2 * j + mine_half), device_id_type=LINK,
        )

    for j in range(pairs):
        p_copy(j).wait_recv()
        z_buf[j] = (y_send[1, j].astype(F32) + p_recv[j].astype(F32)).astype(BF16)
    spread = [
        (lax.rem(g + i, groups), lax.rem(chip + j, pairs))
        for i in range(groups) for j in range(pairs)
    ][1:]
    for a, b in spread:
        y_copy(a, b, g, chip).start()
    y_recv[g, chip] = z_buf[chip, g]
    for a, b in spread[::-1]:
        y_copy(a, b, a, b).wait_recv()
    total = res_buf[t]
    for u in range(groups):
        half = y_recv[u, 0].astype(F32)
        for i in range(1, pairs):
            half = half + y_recv[u, i].astype(F32)
        total = total + weights[u // 2] * half.astype(BF16).astype(F32)
    out_ref[...] = total

    for peer in peers:
        hv_copy(peer, t).wait_send()
        part_copy(peer, t).wait_send()

    x_sends_done()

    for j in range(pairs):
        p_copy(j).wait_send()
    for a, b in spread:
        y_copy(a, b, g, chip).wait_send()


def fused_layer(groups, lanes_tp, *args):
    args = list(args)
    for i in (8, 16, 17):
        args[i] = args[i].T
    for i in (18, 19):
        args[i] = args[i].swapaxes(1, 2)
    args = [a.reshape(1, -1) if a.ndim == 1 and a.dtype == F32 else a for a in args]
    spots = np.arange(HEADS * ROPE) % (ROPE // 2)
    args.append(jnp.asarray((rope_base ** (-2.0 * spots / ROPE))[None].astype(np.float32)))
    rows, width = args[0].shape
    own = args[14].shape[0]
    quarter = width // lanes_tp
    block = HEADS * VDIM // lanes_tp
    local = [
        pltpu.SMEM(a.shape, a.dtype) if i == 14 else pltpu.VMEM(a.shape, a.dtype)
        for i, a in enumerate(args)
    ]
    sem = pltpu.SemaphoreType.DMA
    return pl.pallas_call(
        functools.partial(layer_kernel, groups, lanes_tp),
        out_shape=pltpu.VMEM((rows, quarter), F32),
        in_specs=[pl.BlockSpec(memory_space=pl.ANY)] * len(args),
        out_specs=pl.BlockSpec(memory_space=pltpu.VMEM),
        scratch_shapes=local
        + [
            sem((len(args),)),
            pltpu.VMEM((lanes_tp, 8, block), F32),
            pltpu.VMEM((lanes_tp, 8, block), F32),
            pltpu.VMEM((rows, block), F32),
            pltpu.VMEM((lanes_tp, rows, width), BF16),
            pltpu.VMEM((lanes_tp, rows, quarter), F32),
            pltpu.VMEM((groups, 2, rows, width // 2), BF16),
            pltpu.VMEM((2, lanes_tp // 2, groups, rows, quarter), BF16),
            pltpu.VMEM((lanes_tp // 2, groups, rows, quarter), BF16),
            pltpu.VMEM((lanes_tp // 2, groups, rows, quarter), BF16),
            pltpu.VMEM((groups, lanes_tp // 2, rows, quarter), BF16),
            sem((lanes_tp,)), sem((lanes_tp,)), sem((lanes_tp,)), sem((lanes_tp,)),
            sem((groups,)), sem((groups,)), sem((groups,)), sem((groups,)),
            sem((lanes_tp // 2,)), sem((lanes_tp // 2,)),
            sem((groups, lanes_tp // 2)), sem((groups, lanes_tp // 2)),
        ],
        compiler_params=pltpu.CompilerParams(
            collective_id=0, has_side_effects=True, vmem_limit_bytes=60 * 1024 * 1024
        ),
    )(*args).astype(BF16)


def pick_form(groups, lanes_tp, *args):
    rows = args[0].shape[0]
    if max(2, 4 * rows // (groups // 2)) < rows or lanes_tp % 2:
        return per_device(*args)
    return fused_layer(groups, lanes_tp, *args)


def solution(mesh):
    placed = (
        P("ep", None),
        P(),
        P(),
        P(),
        P(),
        P(),
        P(),
        P(),
        P(),
        P(),
        P(),
        P("tp", None),
        P(("ep", "tp"), None, None),
        P(("ep", "tp"), None, None),
        P(("ep", "tp")),
        P(),
        P("ep", None),
        P("ep", None),
        P("ep", None, "tp"),
        P("ep", None, "tp"),
        P("ep", "tp", None),
    )
    step = functools.partial(pick_form, mesh.shape["ep"], mesh.shape["tp"])
    return jax.shard_map(
        step, mesh=mesh, in_specs=placed, out_specs=P("ep", "tp"), check_vma=False
    )
```
